512 devices in a mesh: kv: 64 (over z, y), tp: 8 (over x, core).
Axes of the slice: x: 4, y: 4, z: 16, core: 2. Of those that a mesh axis runs over, the one named last changes fastest.
Arguments:
- tokens: bfloat16 [256, 2048], P('tp', 'kv'), may hold values from -24 to 24
- lengths: int32 [64], P('kv'), may hold values from 1 to 4, 160 in all
- memory_state: float32 [64, 16, 128, 128], P('kv', 'tp'), may hold values from -3 to 3
- gain_first: float32 [2048], P('kv'), may hold values from 0.1 to 1.9
- first_gate: bfloat16 [2048, 5120], P('kv', 'tp'), may hold values from -0.125 to 0.125
- first_up: bfloat16 [2048, 5120], P('kv', 'tp'), may hold values from -0.125 to 0.125
- first_down: bfloat16 [5120, 2048], P('tp', 'kv'), may hold values from -0.15625 to 0.15625
- gain_mixer: float32 [2048], P('kv'), may hold values from 0.1 to 1.9
- query_weight: bfloat16 [2048, 2048], P('kv', 'tp'), may hold values from -0.125 to 0.125
- key_weight: bfloat16 [2048, 2048], P('kv', 'tp'), may hold values from -0.125 to 0.125
- value_weight: bfloat16 [2048, 2048], P('kv', 'tp'), may hold values from -0.125 to 0.125
- outgate_weight: bfloat16 [2048, 2048], P('kv', 'tp'), may hold values from -0.125 to 0.125
- beta_weight: bfloat16 [2048, 16], P('kv'), may hold values from -0.125 to 0.125
- decay_weight: bfloat16 [2048, 16], P('kv'), may hold values from -0.125 to 0.125
- decay_rate: float32 [16], P('tp'), may hold values from 0.05 to 4
- decay_bias: float32 [16], P('tp'), may hold values from -3 to 1
- head_gain: float32 [128], replicated, may hold values from 0.1 to 1.9
- out_weight: bfloat16 [2048, 2048], P('tp', 'kv'), may hold values from -0.25 to 0.25
- gain_second: float32 [2048], P('kv'), may hold values from 0.1 to 1.9
- second_gate: bfloat16 [2048, 5120], P('kv', 'tp'), may hold values from -0.125 to 0.125
- second_up: bfloat16 [2048, 5120], P('kv', 'tp'), may hold values from -0.125 to 0.125
- second_down: bfloat16 [5120, 2048], P('tp', 'kv'), may hold values from -0.15625 to 0.15625
Outputs:
- layer_out: bfloat16 [256, 2048], P('tp', 'kv')
- state_out: float32 [64, 16, 128, 128], P('kv', 'tp')
The draws below stay inside these ranges and needn't reach their ends.
Inputs may be any that keep to these rules, and one draw needn't show every extreme that they name: `lengths`: each sequence's count of live new token slots.
All inputs are finite; a program needn't handle non-finite values. No bound on the sum of `lengths` on one device may be relied on, other than what follows from the above.
Results may differ from the reference program's by a relative error of at most 0.02.
Values may be sent and summed in bfloat16 or wider, within the bound.
No kernel may reach another device: no remote copies, remote signals or barrier semaphores. Data moves between devices by JAX's collectives and lax.ppermute only.
A program may use at most 64 MiB of HBM per device.

```python
import math
import jax
import jax.numpy as jnp
import numpy as np
from jax import lax

D = 2048
HEADS = 16
HEAD_DIM = 128
FF = 5120
NEW = 4
SEQS = 64
ROWS = 256


def draw_tokens(key, part):
    first_key = jax.random.fold_in(key, 0)
    column = jnp.arange(D, dtype=jnp.float32) / (D - 1)
    column_ramp = jnp.exp(jnp.log(0.5) + column * jnp.log(4.0))
    values = jax.random.normal(first_key, (ROWS, D), jnp.float32) * column_ramp
    return jnp.clip(values, -24.0, 24.0).astype(jnp.bfloat16)


def block_scale(rng, dims, cuts, smallest, high):
    def one(axis_at, parts):
        draws = jax.random.uniform(jax.random.fold_in(jax.random.fold_in(rng, 6), axis_at), (parts,), jnp.float32, smallest / len(cuts), high / len(cuts))
        return jnp.repeat(jnp.exp(draws), dims[axis_at] // parts).reshape((-1,) + (1,) * (len(dims) - axis_at - 1))

    loudness = one(*cuts[0])
    for cut in cuts[1:]:
        loudness = loudness * one(*cut)
    return loudness


def profile(number_of, total, most, slope):
    loads = [(1 << 20) // math.isqrt(grade ** slope) + 1 for grade in range(2, number_of + 1)]
    rest, given = total - most - (number_of - 1), [1] * (number_of - 1)
    while rest > 0:
        movable = [i for i in range(number_of - 1) if given[i] < most]
        pool, left = sum([loads[i] for i in movable]), rest
        for i in movable:
            addition = min(most - given[i], max(1, left * loads[i] // pool), rest)
            given[i] = given[i] + addition
            rest = rest - addition
    return np.array([most] + given)


def ragged(own_key, number_of, total, limit, slope):
    if number_of == 2:
        one = jax.random.randint(own_key, (), max(1, total - limit), min(limit, total - 1) + 1)
        return jnp.stack([one, total - one])
    sizes = jnp.asarray(profile(number_of, total, limit, slope), jnp.int32)
    pairs = (number_of - 1) // 2
    giver, receiver = sizes[1:1 + 2 * pairs:2], sizes[2:2 + 2 * pairs:2]
    margin = jnp.minimum(giver - 1, limit - receiver)
    moved = jax.random.randint(jax.random.fold_in(own_key, 1), (pairs,), 0, 1 << 20) % (margin + 1)
    sizes = sizes.at[1:1 + 2 * pairs:2].set(giver - moved).at[2:2 + 2 * pairs:2].set(receiver + moved)
    return sizes[jax.random.permutation(jax.random.fold_in(own_key, 2), number_of)]


def bell_draw(rng, shape, scale, reach, cuts=(), held_as=jnp.bfloat16):
    array = jax.random.normal(rng, shape, jnp.float32) * scale
    if len(cuts) > 0:
        array = block_scale(rng, shape, cuts, -0.22, 0.18) * array
    return jnp.clip(array, min=-reach, max=reach).astype(held_as)


def setup_inputs(seed: int = 0) -> dict:
    streams_of = jax.random.split(jax.random.key(seed), 23)
    tokens = draw_tokens(jax.random.fold_in(streams_of[22], 71), 0)
    lengths = ragged(streams_of[1], SEQS, (NEW + 1) * SEQS // 2, NEW, 2).astype(jnp.int32)
    memory_state = bell_draw(streams_of[2], (SEQS, HEADS, HEAD_DIM, HEAD_DIM), 0.5, 3.0, ((0, 64), (1, 8)), jnp.float32)
    gain_first = jnp.clip(1.0 + 0.18 * jax.random.normal(streams_of[3], (D,), jnp.float32), 0.1, 1.9)
    first_gate = bell_draw(streams_of[4], (D, FF), D ** -0.5, 0.125, ((0, 64), (1, 8)))
    first_up = bell_draw(streams_of[5], (D, FF), D ** -0.5, 0.125, ((0, 64), (1, 8)))
    first_down = bell_draw(streams_of[6], (FF, D), (FF // 4) ** -0.5, 0.15625, ((0, 8), (1, 64)))
    gain_mixer = jnp.clip(1.0 + 0.18 * jax.random.normal(streams_of[7], (D,), jnp.float32), 0.1, 1.9)
    query_weight = bell_draw(streams_of[8], (D, HEADS * HEAD_DIM), D ** -0.5, 0.125, ((0, 64), (1, 8)))
    key_weight = bell_draw(streams_of[9], (D, HEADS * HEAD_DIM), D ** -0.5, 0.125, ((0, 64), (1, 8)))
    value_weight = bell_draw(streams_of[10], (D, HEADS * HEAD_DIM), D ** -0.5, 0.125, ((0, 64), (1, 8)))
    outgate_weight = bell_draw(streams_of[11], (D, HEADS * HEAD_DIM), D ** -0.5, 0.125, ((0, 64), (1, 8)))
    beta_weight = bell_draw(streams_of[12], (D, HEADS), D ** -0.5, 0.125, ((0, 64),))
    decay_weight = bell_draw(streams_of[13], (D, HEADS), D ** -0.5, 0.125, ((0, 64),))
    decay_rate = jnp.clip(jnp.exp(math.log(4.0) - 4.3820266 * jax.random.uniform(streams_of[14], (HEADS,), jnp.float32) ** block_scale(streams_of[14], (HEADS,), ((0, 8),), -0.2, 0.2)), 0.05, 4.0)
    decay_bias = jnp.clip(-3.0 + 4.0 * jax.random.uniform(streams_of[15], (HEADS,), jnp.float32) ** block_scale(streams_of[15], (HEADS,), ((0, 8),), -0.2, 0.2), -3.0, 1.0)
    head_gain = jnp.clip(1.0 + 0.18 * jax.random.normal(streams_of[16], (HEAD_DIM,), jnp.float32), 0.1, 1.9)
    out_weight = bell_draw(streams_of[17], (HEADS * HEAD_DIM, D), (HEADS * HEAD_DIM // 4) ** -0.5, 0.25, ((0, 8), (1, 64)))
    gain_second = jnp.clip(1.0 + 0.18 * jax.random.normal(streams_of[18], (D,), jnp.float32), 0.1, 1.9)
    second_gate = bell_draw(streams_of[19], (D, FF), D ** -0.5, 0.125, ((0, 64), (1, 8)))
    second_up = bell_draw(streams_of[20], (D, FF), D ** -0.5, 0.125, ((0, 64), (1, 8)))
    second_down = bell_draw(streams_of[21], (FF, D), (FF // 4) ** -0.5, 0.15625, ((0, 8), (1, 64)))
    return {"tokens": tokens, "lengths": lengths, "memory_state": memory_state, "gain_first": gain_first, "first_gate": first_gate, "first_up": first_up, "first_down": first_down, "gain_mixer": gain_mixer, "query_weight": query_weight, "key_weight": key_weight, "value_weight": value_weight, "outgate_weight": outgate_weight, "beta_weight": beta_weight, "decay_weight": decay_weight, "decay_rate": decay_rate, "decay_bias": decay_bias, "head_gain": head_gain, "out_weight": out_weight, "gain_second": gain_second, "second_gate": second_gate, "second_up": second_up, "second_down": second_down}


EPS = 1e-06

def normed_operand(resid, gain):
    widened = resid.astype(jnp.float32)
    squares = lax.optimization_barrier(jnp.sum(widened * widened, axis=1))
    operand = (widened * gain).astype(jnp.bfloat16)
    return (operand, squares)

def inverse_rms(squares):
    return lax.rsqrt(squares / D + EPS)[:, None]

def advance(query_part, key_part, value_part, outgate_part, beta_logit, decay_logit, state_now, lengths, decay_rate, decay_bias, head_gain):
    seqs = state_now.shape[0]
    heads = state_now.shape[1]

    def split_heads(matrix):
        return matrix.reshape(seqs, NEW, heads, HEAD_DIM)
    query = split_heads(jax.nn.silu(query_part))
    query = query * lax.rsqrt(lax.optimization_barrier(jnp.sum(query * query, axis=-1, keepdims=True)) + EPS) * HEAD_DIM ** (-0.5)
    keyvec = split_heads(jax.nn.silu(key_part))
    keyvec = keyvec * lax.rsqrt(lax.optimization_barrier(jnp.sum(keyvec * keyvec, axis=-1, keepdims=True)) + EPS)
    values = split_heads(jax.nn.silu(value_part))
    live_mask = (jnp.arange(NEW, dtype=jnp.int32)[None, :] < lengths[:, None]).astype(jnp.float32)[:, :, None]
    beta_gate = jax.nn.sigmoid(beta_logit.reshape(seqs, NEW, heads)) * live_mask
    decay_log = -decay_rate * jax.nn.softplus(decay_logit.reshape(seqs, NEW, heads) + decay_bias) * live_mask
    outputs = []
    for position in range(NEW):
        state_now = state_now * jnp.exp(decay_log[:, position])[:, :, None, None]
        predicted = jnp.einsum('shk,shkv->shv', keyvec[:, position], state_now, precision=lax.Precision.HIGHEST)
        update = beta_gate[:, position][:, :, None] * (values[:, position] - predicted)
        state_now = state_now + keyvec[:, position][:, :, :, None] * update[:, :, None, :]
        outputs.append(jnp.einsum('shk,shkv->shv', query[:, position], state_now, precision=lax.Precision.HIGHEST))
    mixed = jnp.stack(outputs, axis=1) * live_mask[..., None]
    mixed = mixed * lax.rsqrt(lax.optimization_barrier(jnp.mean(mixed * mixed, axis=-1, keepdims=True)) + EPS) * head_gain
    mixed = mixed * jax.nn.silu(split_heads(outgate_part))
    return (mixed.reshape(seqs * NEW, heads * HEAD_DIM).astype(jnp.bfloat16), state_now)

def channel_mix(resid, gain, w_gate, w_up, w_down):
    operand, squares = normed_operand(resid, gain)
    scale = inverse_rms(squares)
    gate_part = jnp.dot(operand, w_gate, preferred_element_type=jnp.float32) * scale
    up_part = jnp.dot(operand, w_up, preferred_element_type=jnp.float32) * scale
    hidden = (jax.nn.silu(gate_part) * up_part).astype(jnp.bfloat16)
    branch = jnp.dot(hidden, w_down, preferred_element_type=jnp.float32)
    return (resid.astype(jnp.float32) + 0.5 * branch).astype(jnp.bfloat16)

def reference(tokens, lengths, memory_state, gain_first, first_gate, first_up, first_down, gain_mixer, query_weight, key_weight, value_weight, outgate_weight, beta_weight, decay_weight, decay_rate, decay_bias, head_gain, out_weight, gain_second, second_gate, second_up, second_down):
    first = channel_mix(tokens, gain_first, first_gate, first_up, first_down)
    operand, squares = normed_operand(first, gain_mixer)
    scale = inverse_rms(squares)

    def project(weight):
        return jnp.dot(operand, weight, preferred_element_type=jnp.float32) * scale
    mixed, state_out = advance(project(query_weight), project(key_weight), project(value_weight), project(outgate_weight), project(beta_weight), project(decay_weight), memory_state, lengths, decay_rate, decay_bias, head_gain)
    second = (first.astype(jnp.float32) + jnp.dot(mixed, out_weight, preferred_element_type=jnp.float32)).astype(jnp.bfloat16)
    layer_out = channel_mix(second, gain_second, second_gate, second_up, second_down)
    return (layer_out, state_out)
```

```python
import jax
import jax.numpy as jnp
from jax import lax
from jax.sharding import Mesh, PartitionSpec as P

D = 2048
HEAD_DIM = 128
NEW = 4
EPS = 1e-06

NZ, NY, NX, NC = 16, 4, 4, 2
F32 = jnp.float32
BF16 = jnp.bfloat16


def exchange(x, axes):
    return lax.all_to_all(x, axes, 0, 0, tiled=True)


def to_all(x, axes):
    count = lax.axis_size(axes)
    return exchange(jnp.broadcast_to(x[None], (count, *x.shape)), axes)


def dot(a, b):
    return jnp.dot(a, b, preferred_element_type=F32)


def exchange_weights(parts):
    flat = jnp.concatenate([p.reshape(NY, -1) for p in parts], axis=1)
    flat = jnp.pad(flat, ((0, 0), (0, -flat.shape[1] % 1024)))
    width = flat.shape[1]
    both = jnp.broadcast_to(flat[:, None], (NY, NC, width)).reshape(NY * NC, width // 128, 128)
    got = exchange(both, ("y", "c")).reshape(NY, NC, width)
    out, at = [], 0
    for p in parts:
        size = p.shape[1] * p.shape[2]
        out.append(got[:, :, at : at + size].reshape(NY, NC, p.shape[1], p.shape[2]))
        at += size
    return out


def in_three(x):
    first = lax.reduce_precision(x, 8, 7)
    second = lax.reduce_precision(x - first, 8, 7)
    third = x - first - second
    return jnp.concatenate([first, second, third]).astype(BF16)


def up_parts(w):
    return w.reshape(32, NY, 160).transpose(1, 0, 2)


def up_weight(gate, up):
    gate = gate.transpose(0, 2, 1, 3).reshape(128, 320)
    up = up.transpose(0, 2, 1, 3).reshape(128, 320)
    gap = jnp.zeros((128, 64), BF16)
    return jnp.concatenate([gate, gap, up, gap], axis=1)


def down_weight(down):
    down = down.transpose(1, 2, 0, 3).reshape(320, 128)
    return jnp.concatenate([down, jnp.zeros((64, 128), BF16)], axis=0)


def projected(resid, gain, weight, spot):
    wide = resid.astype(F32)
    squares = jnp.sum(wide * wide, axis=1, keepdims=True)
    out = dot((wide * gain[None]).astype(BF16), weight)
    column = lax.broadcasted_iota(jnp.int32, out.shape, 1)
    out = jnp.where(column == spot, squares, out).astype(BF16)
    got = exchange(out.reshape(NZ, 8, -1), "z")
    total = jnp.sum(got.astype(F32), axis=0)
    scale = lax.rsqrt(total[:, spot : spot + 1] / D + EPS)
    return total, scale


def half(resid, gain, w_up, w_down):
    total, scale = projected(resid, gain, w_up, 320)
    hidden = (jax.nn.silu(total[:, :384] * scale) * (total[:, 384:] * scale)).astype(BF16)
    hidden = to_all(hidden, "z").reshape(128, 384)
    return dot(hidden, w_down)


def advance(q, k, v, z, beta_logit, decay_logit, state_now, length, decay_rate, decay_bias, head_gain):
    query = jax.nn.silu(q)
    query = (
        query * lax.rsqrt(jnp.sum(query * query, axis=-1, keepdims=True) + EPS) * HEAD_DIM ** (-0.5)
    )
    keyvec = jax.nn.silu(k)
    keyvec = keyvec * lax.rsqrt(jnp.sum(keyvec * keyvec, axis=-1, keepdims=True) + EPS)
    values = jax.nn.silu(v)
    live = (jnp.arange(NEW, dtype=jnp.int32) < length).astype(F32)[:, None]
    beta = jax.nn.sigmoid(beta_logit) * live
    decay = jnp.exp(-decay_rate * jax.nn.softplus(decay_logit + decay_bias) * live)
    outputs = []
    for t in range(NEW):
        state_now = state_now * decay[t][:, None, None]
        predicted = jnp.sum(keyvec[t][:, :, None] * state_now, axis=1)
        update = beta[t][:, None] * (values[t] - predicted)
        state_now = state_now + keyvec[t][:, :, None] * update[:, None, :]
        outputs.append(jnp.sum(query[t][:, :, None] * state_now, axis=1))
    mixed = jnp.stack(outputs, axis=0) * live[..., None]
    mixed = mixed * lax.rsqrt(jnp.mean(mixed * mixed, axis=-1, keepdims=True) + EPS) * head_gain
    mixed = mixed * jax.nn.silu(z)
    return mixed.reshape(NEW, -1).astype(BF16), state_now


def on_device(
    tokens,
    lengths,
    memory_state,
    gain_first,
    first_gate,
    first_up,
    first_down,
    gain_mixer,
    query_weight,
    key_weight,
    value_weight,
    outgate_weight,
    beta_weight,
    decay_weight,
    decay_rate,
    decay_bias,
    head_gain,
    out_weight,
    gain_second,
    second_gate,
    second_up,
    second_down,
):
    tp = lax.axis_index(("x", "c"))
    logits = jnp.concatenate(
        [
            lax.dynamic_slice_in_dim(beta_weight, tp * 2, 2, 1),
            lax.dynamic_slice_in_dim(decay_weight, tp * 2, 2, 1),
        ],
        axis=1,
    )
    gains = jnp.stack([gain_first, gain_mixer, gain_second])
    parts = [
        up_parts(first_gate),
        up_parts(first_up),
        first_down.reshape(NY, 160, 32),
        jnp.stack([query_weight, key_weight, value_weight, outgate_weight]),
        up_parts(second_gate),
        up_parts(second_up),
        second_down.reshape(NY, 160, 32),
        jnp.broadcast_to(logits[None], (NY, 32, 4)),
        jnp.broadcast_to(in_three(gains)[None], (NY, 9, 32)),
    ]
    gate1, up1, down1, mix, gate2, up2, down2, logit, gains = exchange_weights(parts)
    w_up1, w_down1 = up_weight(gate1, up1), down_weight(down1)
    w_up2, w_down2 = up_weight(gate2, up2), down_weight(down2)
    w_mix = jnp.concatenate(
        [
            mix.transpose(0, 2, 1, 3).reshape(128, 512),
            logit.transpose(0, 2, 1, 3).reshape(128, 8),
            jnp.zeros((128, 120), BF16),
        ],
        axis=1,
    )
    gains = jnp.sum(gains[:, 0].astype(F32).reshape(NY, 3, 3, 32), axis=1)
    gains = gains.transpose(1, 0, 2).reshape(3, 128)

    sent = tokens.reshape(2, NC, 8 * 32).transpose(1, 0, 2).reshape(NC, 512)
    sent = jnp.broadcast_to(sent[None], (NY * NX, NC, 512)).reshape(32, 4, 128)
    got = exchange(sent, ("y", "x", "c")).reshape(NY, NX * NC * 16, 32)
    resid = got.transpose(1, 0, 2).reshape(128, 128)

    branch = half(resid, gains[0], w_up1, w_down1)
    pieces = to_all(branch.astype(BF16), ("y", "x"))
    branch = jnp.sum(pieces.astype(F32), axis=0)
    resid = (resid.astype(F32) + 0.5 * branch).astype(BF16)

    total, scale = projected(resid, gains[1], w_mix, 520)
    total = total * scale
    wide = total[:, :512].reshape(2, NEW, NC, 256).transpose(0, 2, 1, 3)
    small = total[:, 512:520].reshape(2, NEW, NC, 4).transpose(0, 2, 1, 3)
    small = jnp.pad(small, ((0, 0), (0, 0), (0, 0), (0, 124)))
    sent = jnp.concatenate([wide, small], axis=3)
    sent = jnp.broadcast_to(sent[None], (2, 2, NC, NEW, 384)).reshape(NY * NC, 12, 128)
    got = exchange(sent, ("y", "c")).reshape(NY, NC, NEW, 384)
    got = lax.dynamic_index_in_dim(got, lax.axis_index("y") // 2, 1, keepdims=False)
    heads = got[:, :, :256].reshape(4, NEW, 2, HEAD_DIM)
    small = got[0, :, 256:260]
    mixed, state_out = advance(
        heads[0],
        heads[1],
        heads[2],
        heads[3],
        small[:, 0:2],
        small[:, 2:4],
        memory_state[0],
        lengths[0],
        decay_rate,
        decay_bias,
        head_gain,
    )
    everyone = to_all(mixed, ("z", "y"))
    everyone = everyone.reshape(NZ, NC, 8, 256).transpose(1, 0, 2, 3).reshape(NC * 128, 256)
    part = lax.dot_general(
        out_weight, everyone, (((0,), (1,)), ((), ())), preferred_element_type=F32
    ).astype(BF16)
    part = part.reshape(32, NC, 128).transpose(1, 0, 2)
    sent = jnp.broadcast_to(part[None], (NY * NX, NC, 32, 128)).reshape(32, 32, 128)
    got = exchange(sent, ("y", "x", "c")).reshape(NY, NX * NC, 32, 128)
    branch = jnp.sum(got.astype(F32), axis=1).reshape(128, 128).T
    resid = (resid.astype(F32) + branch).astype(BF16)

    branch = half(resid, gains[2], w_up2, w_down2)
    both = jnp.stack([branch.astype(BF16), resid])
    both = both.reshape(2, NX * NC, 16, NY, 32).transpose(3, 1, 0, 2, 4).reshape(32, 8, 128)
    got = exchange(both, ("y", "x", "c")).reshape(NY * NX, NC, 2, 16, 32)
    branch = jnp.sum(got[:, :, 0].astype(F32), axis=0)
    out = (got[0, :, 1].astype(F32) + 0.5 * branch).astype(BF16)
    out = out.reshape(NC, 2, 8, 32).transpose(1, 0, 2, 3).reshape(32, 32)
    return out, state_out[None]


def solution(mesh):
    fine = Mesh(mesh.devices.reshape(NZ, NY, NX, NC), ("z", "y", "x", "c"))
    kv, tp = ("z", "y"), ("x", "c")
    in_specs = (
        P(tp, kv),
        P(kv),
        P(kv, tp, None, None),
        P(kv),
        P(kv, tp),
        P(kv, tp),
        P(tp, kv),
        P(kv),
        P(kv, tp),
        P(kv, tp),
        P(kv, tp),
        P(kv, tp),
        P(kv, None),
        P(kv, None),
        P(tp),
        P(tp),
        P(),
        P(tp, kv),
        P(kv),
        P(kv, tp),
        P(kv, tp),
        P(tp, kv),
    )
    out_specs = (P(tp, kv), P(kv, tp, None, None))
    return jax.shard_map(
        on_device, mesh=fine, in_specs=in_specs, out_specs=out_specs, check_vma=False
    )
```

```python
import jax
import jax.numpy as jnp
from jax import lax
from jax.sharding import Mesh, PartitionSpec as P

D = 2048
HEAD_DIM = 128
NEW = 4
EPS = 1e-06

NZ, NY, NX, NC = 16, 4, 4, 2
F32 = jnp.float32
BF16 = jnp.bfloat16


def exchange(x, axes):
    return lax.all_to_all(x, axes, 0, 0, tiled=True)


def to_all(x, axes):
    count = lax.axis_size(axes)
    return exchange(jnp.broadcast_to(x[None], (count, *x.shape)), axes)


def dot(a, b):
    return jnp.dot(a, b, preferred_element_type=F32)


def in_three(x):
    first = lax.reduce_precision(x, 8, 7)
    second = lax.reduce_precision(x - first, 8, 7)
    third = x - first - second
    return jnp.concatenate([first, second, third], axis=1).astype(BF16)


def gather_weights(pieces):
    own = jnp.concatenate(pieces, axis=1)
    own = jnp.pad(own, ((0, 0), (0, -own.shape[1] % 128)))
    return to_all(own, "y").reshape(128, -1)


def projected(resid, gain, weight, tail):
    wide = resid.astype(F32)
    squares = jnp.sum(wide * wide, axis=1, keepdims=True)
    operand = (wide * gain).astype(BF16)
    out = dot(operand, weight).astype(BF16)
    column = lax.broadcasted_iota(jnp.int32, (64, 128), 1)
    if tail is None:
        last = jnp.where(column == 127, squares, 0.0)
    else:
        last = jnp.where(column == 127, squares, dot(operand, tail))
    out = jnp.concatenate([out, last.astype(BF16)], axis=1)
    got = exchange(out.reshape(NZ, NEW, -1), "z")
    total = jnp.sum(got.astype(F32), axis=0)
    scale = lax.rsqrt(total[:, -1:] / D + EPS)
    return total[:, :-128] * scale, total[:, -128:] * scale


def half(resid, gain, w_up, w_down):
    total, _ = projected(resid, gain, w_up, None)
    hidden = (jax.nn.silu(total[:, :640]) * total[:, 640:]).astype(BF16)
    hidden = to_all(hidden, "z").reshape(64, 640)
    return lax.dot_general(hidden, w_down, (((1,), (1,)), ((), ())), preferred_element_type=F32)


def advance(q, k, v, z, beta_logit, decay_logit, state_now, length, decay_rate, decay_bias, head_gain):
    query = jax.nn.silu(q)
    query = (
        query * lax.rsqrt(jnp.sum(query * query, axis=-1, keepdims=True) + EPS) * HEAD_DIM ** (-0.5)
    )
    keyvec = jax.nn.silu(k)
    keyvec = keyvec * lax.rsqrt(jnp.sum(keyvec * keyvec, axis=-1, keepdims=True) + EPS)
    values = jax.nn.silu(v)
    live = (jnp.arange(NEW, dtype=jnp.int32) < length).astype(F32)[:, None]
    beta = jax.nn.sigmoid(beta_logit) * live
    decay = jnp.exp(-decay_rate * jax.nn.softplus(decay_logit + decay_bias) * live)
    outputs = []
    for t in range(NEW):
        state_now = state_now * decay[t][:, None, None]
        predicted = jnp.sum(keyvec[t][:, :, None] * state_now, axis=1)
        update = beta[t][:, None] * (values[t] - predicted)
        state_now = state_now + keyvec[t][:, :, None] * update[:, None, :]
        outputs.append(jnp.sum(query[t][:, :, None] * state_now, axis=1))
    mixed = jnp.stack(outputs, axis=0) * live[..., None]
    mixed = mixed * lax.rsqrt(jnp.mean(mixed * mixed, axis=-1, keepdims=True) + EPS) * head_gain
    mixed = mixed * jax.nn.silu(z)
    return mixed.reshape(NEW, -1).astype(BF16), state_now


def on_device(
    tokens,
    lengths,
    memory_state,
    gain_first,
    first_gate,
    first_up,
    first_down,
    gain_mixer,
    query_weight,
    key_weight,
    value_weight,
    outgate_weight,
    beta_weight,
    decay_weight,
    decay_rate,
    decay_bias,
    head_gain,
    out_weight,
    gain_second,
    second_gate,
    second_up,
    second_down,
):
    gains = jnp.stack([gain_first, gain_mixer, gain_second], axis=1)
    first = gather_weights([first_gate, first_up, first_down.T, in_three(gains)])
    rest = gather_weights(
        [
            query_weight,
            key_weight,
            value_weight,
            outgate_weight,
            out_weight.T,
            second_gate,
            second_up,
            second_down.T,
            beta_weight,
            decay_weight,
        ]
    )
    gains = jnp.sum(first[:, 1920:1929].astype(F32).T.reshape(3, 3, 128), axis=0)

    sent = tokens.reshape(2, NY, NEW * 32).transpose(1, 0, 2).reshape(NY, 1, 2, 128)
    sent = jnp.broadcast_to(sent, (NY, NX * NC, 2, 128)).reshape(32, 2, 128)
    got = exchange(sent, ("y", "x", "c")).reshape(NY, 64, 32)
    resid = got.transpose(1, 0, 2).reshape(64, 128)

    def over_heads(branch):
        return jnp.sum(to_all(branch.astype(BF16), ("x", "c")).astype(F32), axis=0)

    branch = over_heads(half(resid, gains[0], first[:, :1280], first[:, 1280:1920]))
    resid = (resid.astype(F32) + 0.5 * branch).astype(BF16)

    total, small = projected(resid, gains[1], rest[:, :1024], rest[:, 3200:])
    heads = total.reshape(NEW, 4, 2, HEAD_DIM)
    first_head = 2 * lax.axis_index(("x", "c"))
    mixed, state_out = advance(
        heads[:, 0],
        heads[:, 1],
        heads[:, 2],
        heads[:, 3],
        lax.dynamic_slice_in_dim(small, first_head, 2, 1),
        lax.dynamic_slice_in_dim(small, 16 + first_head, 2, 1),
        memory_state[0],
        lengths[0],
        decay_rate,
        decay_bias,
        head_gain,
    )
    mixed = to_all(mixed, "z").reshape(64, 256)
    branch = over_heads(
        lax.dot_general(
            mixed, rest[:, 1024:1280], (((1,), (1,)), ((), ())), preferred_element_type=F32
        )
    )
    resid = (resid.astype(F32) + branch).astype(BF16)

    branch = half(resid, gains[2], rest[:, 1280:2560], rest[:, 2560:3200])
    both = jnp.stack([branch.astype(BF16), resid])
    both = both.reshape(2, NX * NC, 8, NY, 32).transpose(3, 1, 0, 2, 4).reshape(32, 4, 128)
    got = exchange(both, ("y", "x", "c")).reshape(NY, NX * NC, 2, 8, 32)
    branch = jnp.sum(got[:, :, 0].astype(F32), axis=1)
    out = (got[:, 0, 1].astype(F32) + 0.5 * branch).astype(BF16)
    out = out.reshape(NY, 2, NEW, 32).transpose(1, 0, 2, 3).reshape(32, 32)
    return out, state_out[None]


def solution(mesh):
    fine = Mesh(mesh.devices.reshape(NZ, NY, NX, NC), ("z", "y", "x", "c"))
    kv, tp = ("z", "y"), ("x", "c")
    in_specs = (
        P(tp, kv),
        P(kv),
        P(kv, tp, None, None),
        P(kv),
        P(kv, tp),
        P(kv, tp),
        P(tp, kv),
        P(kv),
        P(kv, tp),
        P(kv, tp),
        P(kv, tp),
        P(kv, tp),
        P(kv, None),
        P(kv, None),
        P(tp),
        P(tp),
        P(),
        P(tp, kv),
        P(kv),
        P(kv, tp),
        P(kv, tp),
        P(tp, kv),
    )
    out_specs = (P(tp, kv), P(kv, tp, None, None))
    return jax.shard_map(
        on_device, mesh=fine, in_specs=in_specs, out_specs=out_specs, check_vma=False
    )
```

```python
import jax
import jax.numpy as jnp
from jax import lax
from jax.sharding import Mesh, PartitionSpec as P

D = 2048
HEAD_DIM = 128
NEW = 4
EPS = 1e-06

NZ, NY, NX, NC = 16, 4, 4, 2
F32 = jnp.float32
BF16 = jnp.bfloat16


def exchange(x, axes):
    return lax.all_to_all(x, axes, 0, 0, tiled=True)


def to_all(x, axes):
    count = lax.axis_size(axes)
    return exchange(jnp.broadcast_to(x[None], (count, *x.shape)), axes)


def dot(a, b):
    return jnp.dot(a, b, preferred_element_type=F32)


def in_three(x):
    first = lax.reduce_precision(x, 8, 7)
    second = lax.reduce_precision(x - first, 8, 7)
    third = x - first - second
    return jnp.concatenate([first, second, third], axis=1).astype(BF16)


def projected(resid, gain, weight, tail):
    wide = resid.astype(F32)
    squares = jnp.sum(wide * wide, axis=1, keepdims=True)
    operand = (wide * gain).astype(BF16)
    out = dot(operand, weight).astype(BF16)
    column = lax.broadcasted_iota(jnp.int32, (64, 128), 1)
    if tail is None:
        last = jnp.where(column == 127, squares, 0.0)
    else:
        last = jnp.where(column == 127, squares, dot(operand, tail))
    out = jnp.concatenate([out, last.astype(BF16)], axis=1)
    got = exchange(out.reshape(NZ, NEW, -1), "z")
    total = jnp.sum(got.astype(F32), axis=0)
    scale = lax.rsqrt(total[:, -1:] / D + EPS)
    return total[:, :-128] * scale, total[:, -128:] * scale


def half(resid, gain, w_up, w_down):
    total, _ = projected(resid, gain, w_up, None)
    hidden = (jax.nn.silu(total[:, :640]) * total[:, 640:]).astype(BF16)
    hidden = to_all(hidden, "z").reshape(64, 640)
    return lax.dot_general(hidden, w_down, (((1,), (1,)), ((), ())), preferred_element_type=F32)


def advance(q, k, v, z, beta_logit, decay_logit, state_now, length, decay_rate, decay_bias, head_gain):
    query = jax.nn.silu(q)
    query = (
        query * lax.rsqrt(jnp.sum(query * query, axis=-1, keepdims=True) + EPS) * HEAD_DIM ** (-0.5)
    )
    keyvec = jax.nn.silu(k)
    keyvec = keyvec * lax.rsqrt(jnp.sum(keyvec * keyvec, axis=-1, keepdims=True) + EPS)
    values = jax.nn.silu(v)
    live = (jnp.arange(NEW, dtype=jnp.int32) < length).astype(F32)[:, None]
    beta = jax.nn.sigmoid(beta_logit) * live
    decay = jnp.exp(-decay_rate * jax.nn.softplus(decay_logit + decay_bias) * live)
    outputs = []
    for t in range(NEW):
        state_now = state_now * decay[t][:, None, None]
        predicted = jnp.sum(keyvec[t][:, :, None] * state_now, axis=1)
        update = beta[t][:, None] * (values[t] - predicted)
        state_now = state_now + keyvec[t][:, :, None] * update[:, None, :]
        outputs.append(jnp.sum(query[t][:, :, None] * state_now, axis=1))
    mixed = jnp.stack(outputs, axis=0) * live[..., None]
    mixed = mixed * lax.rsqrt(jnp.mean(mixed * mixed, axis=-1, keepdims=True) + EPS) * head_gain
    mixed = mixed * jax.nn.silu(z)
    return mixed.reshape(NEW, -1).astype(BF16), state_now


def on_device(
    tokens,
    lengths,
    memory_state,
    gain_first,
    first_gate,
    first_up,
    first_down,
    gain_mixer,
    query_weight,
    key_weight,
    value_weight,
    outgate_weight,
    beta_weight,
    decay_weight,
    decay_rate,
    decay_bias,
    head_gain,
    out_weight,
    gain_second,
    second_gate,
    second_up,
    second_down,
):
    weights = [
        first_gate,
        first_up,
        first_down.T,
        query_weight,
        key_weight,
        value_weight,
        outgate_weight,
        out_weight.T,
        second_gate,
        second_up,
        second_down.T,
    ]
    gains = jnp.stack([gain_first, gain_mixer, gain_second], axis=1)
    tail = [beta_weight, decay_weight, in_three(gains), jnp.zeros((32, 75), BF16)]
    own = jnp.concatenate([*weights, *tail], axis=1)
    sent = tokens.T.reshape(32, 2, NY, NEW).transpose(2, 0, 1, 3).reshape(NY, 32, 8)
    sent = jnp.pad(sent, ((0, 0), (0, 0), (0, 4)))
    own = jnp.broadcast_to(own[None], (NY, *own.shape))
    near = exchange(jnp.concatenate([own, sent], axis=2), "y").reshape(128, 5248)
    w_up1, w_down1 = near[:, :1280], near[:, 1280:1920]
    w_mix, w_out = near[:, 1920:2944], near[:, 2944:3200]
    w_up2, w_down2 = near[:, 3200:4480], near[:, 4480:5120]
    tail = near[:, 5120:]
    gains = jnp.sum(tail[:, 32:41].astype(F32).T.reshape(3, 3, 128), axis=0)
    resid = to_all(tail[:, 116:124].T, ("x", "c")).reshape(64, 128)

    def over_heads(branch):
        return jnp.sum(to_all(branch.astype(BF16), ("x", "c")).astype(F32), axis=0)

    branch = over_heads(half(resid, gains[0], w_up1, w_down1))
    resid = (resid.astype(F32) + 0.5 * branch).astype(BF16)

    total, small = projected(resid, gains[1], w_mix, tail)
    heads = total.reshape(NEW, 4, 2, HEAD_DIM)
    first_head = 2 * lax.axis_index(("x", "c"))
    mixed, state_out = advance(
        heads[:, 0],
        heads[:, 1],
        heads[:, 2],
        heads[:, 3],
        lax.dynamic_slice_in_dim(small, first_head, 2, 1),
        lax.dynamic_slice_in_dim(small, 16 + first_head, 2, 1),
        memory_state[0],
        lengths[0],
        decay_rate,
        decay_bias,
        head_gain,
    )
    mixed = to_all(mixed, "z").reshape(64, 256)
    branch = over_heads(
        lax.dot_general(mixed, w_out, (((1,), (1,)), ((), ())), preferred_element_type=F32)
    )
    resid = (resid.astype(F32) + branch).astype(BF16)

    branch = half(resid, gains[2], w_up2, w_down2)
    both = jnp.stack([branch.astype(BF16), resid])
    both = both.reshape(2, NX * NC, 8, NY, 32).transpose(3, 1, 0, 2, 4).reshape(32, 4, 128)
    got = exchange(both, ("y", "x", "c")).reshape(NY, NX * NC, 2, 8, 32)
    branch = jnp.sum(got[:, :, 0].astype(F32), axis=1)
    out = (got[:, 0, 1].astype(F32) + 0.5 * branch).astype(BF16)
    out = out.reshape(NY, 2, NEW, 32).transpose(1, 0, 2, 3).reshape(32, 32)
    return out, state_out[None]


def solution(mesh):
    fine = Mesh(mesh.devices.reshape(NZ, NY, NX, NC), ("z", "y", "x", "c"))
    kv, tp = ("z", "y"), ("x", "c")
    in_specs = (
        P(tp, kv),
        P(kv),
        P(kv, tp, None, None),
        P(kv),
        P(kv, tp),
        P(kv, tp),
        P(tp, kv),
        P(kv),
        P(kv, tp),
        P(kv, tp),
        P(kv, tp),
        P(kv, tp),
        P(kv, None),
        P(kv, None),
        P(tp),
        P(tp),
        P(),
        P(tp, kv),
        P(kv),
        P(kv, tp),
        P(kv, tp),
        P(tp, kv),
    )
    out_specs = (P(tp, kv), P(kv, tp, None, None))
    return jax.shard_map(
        on_device, mesh=fine, in_specs=in_specs, out_specs=out_specs, check_vma=False
    )
```

```python
import jax
import jax.numpy as jnp
from jax import lax
from jax.experimental import pallas as pl
from jax.experimental.pallas import tpu as pltpu
from jax.sharding import Mesh, PartitionSpec as P

D = 2048
HEAD_DIM = 128
NEW = 4
EPS = 1e-06

NZ, NY, NX, NC = 16, 4, 4, 2
F32 = jnp.float32
BF16 = jnp.bfloat16


def exchange(x, axes):
    return lax.all_to_all(x, axes, 0, 0, tiled=True)


def to_all(x, axes):
    count = lax.axis_size(axes)
    return exchange(jnp.broadcast_to(x[None], (count, *x.shape)), axes)


def dot(a, b):
    return jnp.dot(a, b, preferred_element_type=F32)


def projected(resid, gain, weight, tail):
    wide = resid.astype(F32)
    squares = jnp.sum(wide * wide, axis=1, keepdims=True)
    operand = (wide * gain).astype(BF16)
    last = jnp.concatenate([dot(operand, tail)[:, :127], squares], axis=1)
    out = jnp.concatenate([dot(operand, weight).astype(BF16), last.astype(BF16)], axis=1)
    return exchange(out.reshape(NZ, NEW, -1), "z")


def summed(got):
    total = jnp.sum(got.astype(F32), axis=0)
    scale = lax.rsqrt(total[:, -1:] / D + EPS)
    return total[:, :-128] * scale, total[:, -128:] * scale


def half(resid, gain, w_up, w_down, tail):
    total, _ = summed(projected(resid, gain, w_up, tail))
    hidden = (jax.nn.silu(total[:, :640]) * total[:, 640:]).astype(BF16)
    hidden = to_all(hidden, "z").reshape(64, 640)
    return lax.dot_general(hidden, w_down, (((1,), (1,)), ((), ())), preferred_element_type=F32)


def advance(q, k, v, z, beta_logit, decay_logit, state_now, live, decay_rate, decay_bias, head_gain):
    query = jax.nn.silu(q)
    query = (
        query * lax.rsqrt(jnp.sum(query * query, axis=-1, keepdims=True) + EPS) * HEAD_DIM ** (-0.5)
    )
    keyvec = jax.nn.silu(k)
    keyvec = keyvec * lax.rsqrt(jnp.sum(keyvec * keyvec, axis=-1, keepdims=True) + EPS)
    values = jax.nn.silu(v)
    beta = jax.nn.sigmoid(beta_logit) * live
    decay = jnp.exp(-decay_rate * jax.nn.softplus(decay_logit + decay_bias) * live)
    outputs = []
    for t in range(NEW):
        state_now = state_now * decay[t][:, None, None]
        predicted = jnp.sum(keyvec[t][:, :, None] * state_now, axis=1)
        update = beta[t][:, None] * (values[t] - predicted)
        state_now = state_now + keyvec[t][:, :, None] * update[:, None, :]
        outputs.append(jnp.sum(query[t][:, :, None] * state_now, axis=1))
    mixed = jnp.stack(outputs, axis=0) * live[..., None]
    mixed = mixed * lax.rsqrt(jnp.mean(mixed * mixed, axis=-1, keepdims=True) + EPS) * head_gain
    mixed = mixed * jax.nn.silu(z)
    return mixed.reshape(NEW, -1).astype(BF16), state_now


def pack_kernel(*refs):
    length_ref, tokens_ref, *refs = refs
    gain_refs, logit_refs, weight_refs = refs[:3], refs[3:5], refs[5:-2]
    out_ref, live_ref = refs[-2:]
    slot = lax.broadcasted_iota(jnp.int32, (NEW, 128), 0)
    live_ref[...] = (slot < length_ref[0]).astype(F32)
    at = 0
    for ref in weight_refs:
        block = ref[...]
        for y in range(NY):
            out_ref[y, :, at : at + block.shape[1]] = block
        at += block.shape[1]
    gains = jnp.concatenate([ref[...] for ref in gain_refs], axis=0)
    first = gains.astype(BF16).astype(F32)
    second = (gains - first).astype(BF16).astype(F32)
    third = gains - first - second
    device = NC * lax.axis_index("x") + lax.axis_index("c")
    row = lax.broadcasted_iota(jnp.int32, (16, 32), 0)
    logits = []
    for ref in logit_refs:
        block = ref[...].astype(F32)
        for h in range(2):
            mine = jnp.where(row == 2 * device + h, block, 0.0)
            logits.append(jnp.sum(mine, axis=0, keepdims=True))
    gap = jnp.zeros((3, 32), F32)
    small = jnp.concatenate([*logits, first, second, third, gap], axis=0)
    rows = tokens_ref[...].astype(F32)
    end = jnp.zeros((104, 32), F32)
    for y in range(NY):
        mine = [rows[4 * y : 4 * y + 4], rows[16 + 4 * y : 20 + 4 * y]]
        tail = jnp.concatenate([small, *mine, end], axis=0)
        out_ref[y, :, at:] = tail.T.astype(BF16)


def pack(lengths, tokens, gains, logits, weights):
    gains = [g.reshape(1, 32) for g in gains]
    logits = [w.T for w in logits]
    space = pl.BlockSpec(memory_space=pltpu.VMEM)
    return pl.pallas_call(
        pack_kernel,
        out_shape=[
            jax.ShapeDtypeStruct((NY, 32, 5248), BF16),
            jax.ShapeDtypeStruct((NEW, 128), F32),
        ],
        in_specs=[pl.BlockSpec(memory_space=pltpu.SMEM)] + [space] * (6 + len(weights)),
        out_specs=[space, space],
        name="pack",
    )(lengths, tokens, *gains, *logits, *weights)


def on_device(
    tokens,
    lengths,
    memory_state,
    gain_first,
    first_gate,
    first_up,
    first_down,
    gain_mixer,
    query_weight,
    key_weight,
    value_weight,
    outgate_weight,
    beta_weight,
    decay_weight,
    decay_rate,
    decay_bias,
    head_gain,
    out_weight,
    gain_second,
    second_gate,
    second_up,
    second_down,
):
    near, live = pack(
        lengths,
        tokens,
        [gain_first, gain_mixer, gain_second],
        [beta_weight, decay_weight],
        [
            first_gate,
            first_up,
            first_down.T,
            query_weight,
            key_weight,
            value_weight,
            outgate_weight,
            out_weight.T,
            second_gate,
            second_up,
            second_down.T,
        ],
    )
    near = exchange(near, "y").reshape(128, 5248)
    w_up1, w_down1 = near[:, :1280], near[:, 1280:1920]
    w_mix, w_out = near[:, 1920:2944], near[:, 2944:3200]
    w_up2, w_down2 = near[:, 3200:4480], near[:, 4480:5120]
    tail = near[:, 5120:]
    got = to_all(tail[:, :32].T, ("x", "c"))
    resid = got[:, 16:24].reshape(64, 128)
    gains = jnp.sum(got[0, 4:13].astype(F32).reshape(3, 3, 128), axis=0)

    def over_heads(branch):
        return jnp.sum(to_all(branch.astype(BF16), ("x", "c")).astype(F32), axis=0)

    branch = over_heads(half(resid, gains[0], w_up1, w_down1, tail))
    resid = (resid.astype(F32) + 0.5 * branch).astype(BF16)

    got = projected(resid, gains[1], w_mix, tail)
    total, small = summed(got)
    heads = total.reshape(NEW, 4, 2, HEAD_DIM)
    mixed, state_out = advance(
        heads[:, 0],
        heads[:, 1],
        heads[:, 2],
        heads[:, 3],
        small[:, 0:2],
        small[:, 2:4],
        memory_state[0],
        live[:, :1],
        decay_rate,
        decay_bias,
        head_gain,
    )
    mixed, state_out = lax.optimization_barrier((mixed, state_out))
    mixed = to_all(mixed, "z").reshape(64, 256)
    branch = over_heads(
        lax.dot_general(mixed, w_out, (((1,), (1,)), ((), ())), preferred_element_type=F32)
    )
    resid = (resid.astype(F32) + branch).astype(BF16)

    branch = half(resid, gains[2], w_up2, w_down2, tail)
    branch, resid = lax.optimization_barrier((branch, resid))
    both = jnp.stack([branch.astype(BF16), resid])
    both = both.reshape(2, NX * NC, 8, NY, 32).transpose(3, 1, 0, 2, 4).reshape(32, 4, 128)
    got = exchange(both, ("y", "x", "c")).reshape(NY, NX * NC, 2, 8, 32)
    branch = jnp.sum(got[:, :, 0].astype(F32), axis=1)
    out = (got[:, 0, 1].astype(F32) + 0.5 * branch).astype(BF16)
    out = out.reshape(NY, 2, NEW, 32).transpose(1, 0, 2, 3).reshape(32, 32)
    return out, state_out[None]


def solution(mesh):
    fine = Mesh(mesh.devices.reshape(NZ, NY, NX, NC), ("z", "y", "x", "c"))
    kv, tp = ("z", "y"), ("x", "c")
    in_specs = (
        P(tp, kv),
        P(kv),
        P(kv, tp, None, None),
        P(kv),
        P(kv, tp),
        P(kv, tp),
        P(tp, kv),
        P(kv),
        P(kv, tp),
        P(kv, tp),
        P(kv, tp),
        P(kv, tp),
        P(kv, None),
        P(kv, None),
        P(tp),
        P(tp),
        P(),
        P(tp, kv),
        P(kv),
        P(kv, tp),
        P(kv, tp),
        P(tp, kv),
    )
    out_specs = (P(tp, kv), P(kv, tp, None, None))
    return jax.shard_map(
        on_device, mesh=fine, in_specs=in_specs, out_specs=out_specs, check_vma=False
    )
```

```python
import jax
import jax.numpy as jnp
from jax import lax
from jax.experimental import pallas as pl
from jax.experimental.pallas import tpu as pltpu
from jax.sharding import Mesh, PartitionSpec as P

D = 2048
HEAD_DIM = 128
NEW = 4
EPS = 1e-06

NZ, NY, NX, NC = 16, 4, 4, 2
F32 = jnp.float32
BF16 = jnp.bfloat16


def exchange(x, axes):
    return lax.all_to_all(x, axes, 0, 0, tiled=True)


def to_all(x, axes):
    count = lax.axis_size(axes)
    return exchange(jnp.broadcast_to(x[None], (count, *x.shape)), axes)


def dot(a, b):
    return jnp.dot(a, b, preferred_element_type=F32)


def projected(resid, gain, weight, tail):
    wide = resid.astype(F32)
    squares = jnp.sum(wide * wide, axis=1, keepdims=True)
    operand = (wide * gain).astype(BF16)
    last = jnp.concatenate([dot(operand, tail)[:, :127], squares], axis=1)
    out = jnp.concatenate([dot(operand, weight).astype(BF16), last.astype(BF16)], axis=1)
    return exchange(out.reshape(NZ, NEW, -1), "z")


def summed(got):
    total = jnp.sum(got.astype(F32), axis=0)
    scale = lax.rsqrt(total[:, -1:] / D + EPS)
    return total[:, :-128] * scale, total[:, -128:] * scale


def half(resid, gain, w_up, w_down, tail):
    total, _ = summed(projected(resid, gain, w_up, tail))
    hidden = (jax.nn.silu(total[:, :640]) * total[:, 640:]).astype(BF16)
    hidden = to_all(hidden, "z").reshape(64, 640)
    return lax.dot_general(hidden, w_down, (((1,), (1,)), ((), ())), preferred_element_type=F32)


def advance(q, k, v, z, beta_logit, decay_logit, state_now, live, decay_rate, decay_bias, head_gain):
    query = jax.nn.silu(q)
    query = (
        query * lax.rsqrt(jnp.sum(query * query, axis=-1, keepdims=True) + EPS) * HEAD_DIM ** (-0.5)
    )
    keyvec = jax.nn.silu(k)
    keyvec = keyvec * lax.rsqrt(jnp.sum(keyvec * keyvec, axis=-1, keepdims=True) + EPS)
    values = jax.nn.silu(v)
    beta = jax.nn.sigmoid(beta_logit) * live
    decay = jnp.exp(decay_rate * jax.nn.softplus(decay_logit + decay_bias))
    outputs = []
    for t in range(NEW):
        state_now = state_now * decay[t][:, None, None]
        predicted = jnp.sum(keyvec[t][:, :, None] * state_now, axis=1)
        update = beta[t][:, None] * (values[t] - predicted)
        state_now = state_now + keyvec[t][:, :, None] * update[:, None, :]
        outputs.append(jnp.sum(query[t][:, :, None] * state_now, axis=1))
    mixed = jnp.stack(outputs, axis=0) * live[:, :, None]
    mixed = mixed * lax.rsqrt(jnp.mean(mixed * mixed, axis=-1, keepdims=True) + EPS) * head_gain
    mixed = mixed * jax.nn.silu(z)
    return mixed.reshape(NEW, -1).astype(BF16), state_now


def pack_kernel(*refs):
    length_ref, rate_ref, bias_ref, head_gain_ref, tokens_ref, *refs = refs
    gain_refs, logit_refs, weight_refs = refs[:3], refs[3:5], refs[5:-5]
    out_ref, live_ref, minus_ref, wide_bias_ref, wide_gain_ref = refs[-5:]
    slot = lax.broadcasted_iota(jnp.int32, (NEW, 2), 0)
    live = (slot < jnp.broadcast_to(length_ref[...], (NEW, 2))).astype(F32)
    live_ref[...] = live
    minus_ref[...] = -rate_ref[...] * live
    wide_bias_ref[...] = jnp.broadcast_to(bias_ref[...], (NEW, 2))
    for t in range(NEW):
        wide_gain_ref[t] = jnp.broadcast_to(head_gain_ref[...], (2, HEAD_DIM))
    at = 0
    for ref in weight_refs:
        block = ref[...]
        for y in range(NY):
            out_ref[y, :, at : at + block.shape[1]] = block
        at += block.shape[1]
    gains = jnp.concatenate([ref[...] for ref in gain_refs], axis=0)
    first = gains.astype(BF16).astype(F32)
    second = (gains - first).astype(BF16).astype(F32)
    third = gains - first - second
    device = NC * lax.axis_index("x") + lax.axis_index("c")
    row = lax.broadcasted_iota(jnp.int32, (16, 32), 0)
    logits = []
    for ref in logit_refs:
        block = ref[...].astype(F32)
        for h in range(2):
            mine = jnp.where(row == 2 * device + h, block, 0.0)
            logits.append(jnp.sum(mine, axis=0, keepdims=True))
    gap = jnp.zeros((3, 32), F32)
    small = jnp.concatenate([*logits, first, second, third, gap], axis=0)
    rows = tokens_ref[...].astype(F32)
    end = jnp.zeros((104, 32), F32)
    for y in range(NY):
        mine = [rows[4 * y : 4 * y + 4], rows[16 + 4 * y : 20 + 4 * y]]
        tail = jnp.concatenate([small, *mine, end], axis=0)
        out_ref[y, :, at:] = tail.T.astype(BF16)


def pack(scalars, tokens, gains, logits, weights):
    gains = [g.reshape(1, 32) for g in gains]
    logits = [w.T for w in logits]
    space = pl.BlockSpec(memory_space=pltpu.VMEM)
    return pl.pallas_call(
        pack_kernel,
        out_shape=[
            jax.ShapeDtypeStruct((NY, 32, 5248), BF16),
            jax.ShapeDtypeStruct((NEW, 2), F32),
            jax.ShapeDtypeStruct((NEW, 2), F32),
            jax.ShapeDtypeStruct((NEW, 2), F32),
            jax.ShapeDtypeStruct((NEW, 2, HEAD_DIM), F32),
        ],
        in_specs=[space] * (10 + len(weights)),
        out_specs=[space] * 5,
        name="pack",
    )(*(v.reshape(1, -1) for v in scalars), tokens, *gains, *logits, *weights)


def on_device(
    tokens,
    lengths,
    memory_state,
    gain_first,
    first_gate,
    first_up,
    first_down,
    gain_mixer,
    query_weight,
    key_weight,
    value_weight,
    outgate_weight,
    beta_weight,
    decay_weight,
    decay_rate,
    decay_bias,
    head_gain,
    out_weight,
    gain_second,
    second_gate,
    second_up,
    second_down,
):
    near, live, rate, bias, wide_gain = pack(
        [lengths, decay_rate, decay_bias, head_gain],
        tokens,
        [gain_first, gain_mixer, gain_second],
        [beta_weight, decay_weight],
        [
            first_gate,
            first_up,
            first_down.T,
            query_weight,
            key_weight,
            value_weight,
            outgate_weight,
            out_weight.T,
            second_gate,
            second_up,
            second_down.T,
        ],
    )
    near = exchange(near, "y").reshape(128, 5248)
    w_up1, w_down1 = near[:, :1280], near[:, 1280:1920]
    w_mix, w_out = near[:, 1920:2944], near[:, 2944:3200]
    w_up2, w_down2 = near[:, 3200:4480], near[:, 4480:5120]
    tail = near[:, 5120:]
    got = to_all(tail[:, :32].T, ("x", "c"))
    resid = got[:, 16:24].reshape(64, 128)
    gains = jnp.sum(got[0, 4:13].astype(F32).reshape(3, 3, 128), axis=0)

    def over_heads(branch):
        return jnp.sum(to_all(branch.astype(BF16), ("x", "c")).astype(F32), axis=0)

    branch = over_heads(half(resid, gains[0], w_up1, w_down1, tail))
    resid = (resid.astype(F32) + 0.5 * branch).astype(BF16)

    got = projected(resid, gains[1], w_mix, tail)
    total, small = summed(got)
    heads = total.reshape(NEW, 4, 2, HEAD_DIM)
    mixed, state_out = advance(
        heads[:, 0],
        heads[:, 1],
        heads[:, 2],
        heads[:, 3],
        small[:, 0:2],
        small[:, 2:4],
        memory_state[0],
        live,
        rate,
        bias,
        wide_gain,
    )
    mixed, state_out = lax.optimization_barrier((mixed, state_out))
    mixed = to_all(mixed, "z").reshape(64, 256)
    branch = over_heads(
        lax.dot_general(mixed, w_out, (((1,), (1,)), ((), ())), preferred_element_type=F32)
    )
    resid = (resid.astype(F32) + branch).astype(BF16)

    branch = half(resid, gains[2], w_up2, w_down2, tail)
    branch, resid = lax.optimization_barrier((branch, resid))
    both = jnp.stack([branch.astype(BF16), resid])
    both = both.reshape(2, NX * NC, 8, NY, 32).transpose(3, 1, 0, 2, 4).reshape(32, 4, 128)
    got = exchange(both, ("y", "x", "c")).reshape(NY, NX * NC, 2, 8, 32)
    branch = jnp.sum(got[:, :, 0].astype(F32), axis=1)
    out = (got[:, 0, 1].astype(F32) + 0.5 * branch).astype(BF16)
    out = out.reshape(NY, 2, NEW, 32).transpose(1, 0, 2, 3).reshape(32, 32)
    return out, state_out[None]


def solution(mesh):
    fine = Mesh(mesh.devices.reshape(NZ, NY, NX, NC), ("z", "y", "x", "c"))
    kv, tp = ("z", "y"), ("x", "c")
    in_specs = (
        P(tp, kv),
        P(kv),
        P(kv, tp, None, None),
        P(kv),
        P(kv, tp),
        P(kv, tp),
        P(tp, kv),
        P(kv),
        P(kv, tp),
        P(kv, tp),
        P(kv, tp),
        P(kv, tp),
        P(kv, None),
        P(kv, None),
        P(tp),
        P(tp),
        P(),
        P(tp, kv),
        P(kv),
        P(kv, tp),
        P(kv, tp),
        P(tp, kv),
    )
    out_specs = (P(tp, kv), P(kv, tp, None, None))
    return jax.shard_map(
        on_device, mesh=fine, in_specs=in_specs, out_specs=out_specs, check_vma=False
    )
```

```python
import jax
import jax.numpy as jnp
from jax import lax
from jax.experimental import pallas as pl
from jax.experimental.pallas import tpu as pltpu
from jax.sharding import Mesh, PartitionSpec as P

D = 2048
HEAD_DIM = 128
NEW = 4
EPS = 1e-06


NZ, NY, NX, NC = 16, 4, 4, 2
F32 = jnp.float32
BF16 = jnp.bfloat16


def exchange(x, axes):
    return lax.all_to_all(x, axes, 0, 0, tiled=True)


def to_all(x, axes):
    count = lax.axis_size(axes)
    return exchange(jnp.broadcast_to(x[None], (count, *x.shape)), axes)


def dot(a, b):
    return jnp.dot(a, b, preferred_element_type=F32)


def projected(resid, gain, weight, tail):
    wide = resid.astype(F32)
    squares = jnp.sum(wide * wide, axis=1, keepdims=True)
    operand = (wide * gain).astype(BF16)
    last = jnp.concatenate([dot(operand, tail)[:, :127], squares], axis=1)
    out = jnp.concatenate([dot(operand, weight).astype(BF16), last.astype(BF16)], axis=1)
    return exchange(out.reshape(NZ, NEW, -1), "z")


def summed(got):
    total = jnp.sum(got.astype(F32), axis=0)
    scale = lax.rsqrt(total[:, -1:] / D + EPS)
    return total[:, :-128] * scale, total[:, -128:] * scale


def half(resid, gain, w_up, w_down, tail):
    total, _ = summed(projected(resid, gain, w_up, tail))
    hidden = (jax.nn.silu(total[:, :640]) * total[:, 640:]).astype(BF16)
    hidden = to_all(hidden, "z").reshape(64, 640)
    return lax.dot_general(hidden, w_down, (((1,), (1,)), ((), ())), preferred_element_type=F32)


def advance(q, k, v, z, beta_logit, decay_logit, state_now, live, decay_rate, decay_bias, head_gain):
    query = jax.nn.silu(q)
    query = (
        query * lax.rsqrt(jnp.sum(query * query, axis=-1, keepdims=True) + EPS) * HEAD_DIM ** (-0.5)
    )
    keyvec = jax.nn.silu(k)
    keyvec = keyvec * lax.rsqrt(jnp.sum(keyvec * keyvec, axis=-1, keepdims=True) + EPS)
    values = jax.nn.silu(v)
    beta = jax.nn.sigmoid(beta_logit) * live
    decay = jnp.exp(decay_rate * jax.nn.softplus(decay_logit + decay_bias))
    outputs = []
    for t in range(NEW):
        state_now = state_now * decay[t][:, None, None]
        predicted = jnp.sum(keyvec[t][:, :, None] * state_now, axis=1)
        update = beta[t][:, None] * (values[t] - predicted)
        state_now = state_now + keyvec[t][:, :, None] * update[:, None, :]
        outputs.append(jnp.sum(query[t][:, :, None] * state_now, axis=1))
    mixed = jnp.stack(outputs, axis=0) * live[:, :, None]
    mixed = mixed * lax.rsqrt(jnp.mean(mixed * mixed, axis=-1, keepdims=True) + EPS) * head_gain
    mixed = mixed * jax.nn.silu(z)
    return mixed.reshape(NEW, -1).astype(BF16), state_now


def from_others(own):
    blocks = [own]
    for d in range(1, NY):
        blocks.append(lax.ppermute(own, "y", [(y, y ^ d) for y in range(NY)]))
    here = lax.axis_index("y")
    return jnp.concatenate([lax.select_n(here ^ y, *blocks) for y in range(NY)], axis=0)


def pack_kernel(*refs):
    length_ref, rate_ref, bias_ref, head_gain_ref, tokens_ref, *refs = refs
    gain_refs, logit_refs, weight_refs = refs[:3], refs[3:5], refs[5:-6]
    out_ref, far_ref, live_ref, minus_ref, wide_bias_ref, wide_gain_ref = refs[-6:]
    slot = lax.broadcasted_iota(jnp.int32, (NEW, 2), 0)
    live = (slot < jnp.broadcast_to(length_ref[...], (NEW, 2))).astype(F32)
    live_ref[...] = live
    minus_ref[...] = -rate_ref[...] * live
    wide_bias_ref[...] = jnp.broadcast_to(bias_ref[...], (NEW, 2))
    for t in range(NEW):
        wide_gain_ref[t] = jnp.broadcast_to(head_gain_ref[...], (2, HEAD_DIM))
    at = 0
    for ref in weight_refs[3:]:
        far_ref[:, at : at + ref.shape[1]] = ref[...]
        at += ref.shape[1]
    at = 0
    for ref in weight_refs[:3]:
        block = ref[...]
        for y in range(NY):
            out_ref[y, :, at : at + block.shape[1]] = block
        at += block.shape[1]
    gains = jnp.concatenate([ref[...] for ref in gain_refs], axis=0)
    first = gains.astype(BF16).astype(F32)
    second = (gains - first).astype(BF16).astype(F32)
    third = gains - first - second
    device = NC * lax.axis_index("x") + lax.axis_index("c")
    row = lax.broadcasted_iota(jnp.int32, (16, 32), 0)
    logits = []
    for ref in logit_refs:
        block = ref[...].astype(F32)
        for h in range(2):
            mine = jnp.where(row == 2 * device + h, block, 0.0)
            logits.append(jnp.sum(mine, axis=0, keepdims=True))
    gap = jnp.zeros((3, 32), F32)
    small = jnp.concatenate([*logits, first, second, third, gap], axis=0)
    rows = tokens_ref[...].astype(F32)
    end = jnp.zeros((104, 32), F32)
    for y in range(NY):
        mine = [rows[4 * y : 4 * y + 4], rows[16 + 4 * y : 20 + 4 * y]]
        tail = jnp.concatenate([small, *mine, end], axis=0)
        out_ref[y, :, at:] = tail.T.astype(BF16)


def pack(scalars, tokens, gains, logits, weights):
    gains = [g.reshape(1, 32) for g in gains]
    logits = [w.T for w in logits]
    space = pl.BlockSpec(memory_space=pltpu.VMEM)
    return pl.pallas_call(
        pack_kernel,
        out_shape=[
            jax.ShapeDtypeStruct((NY, 32, 2048), BF16),
            jax.ShapeDtypeStruct((32, 3200), BF16),
            jax.ShapeDtypeStruct((NEW, 2), F32),
            jax.ShapeDtypeStruct((NEW, 2), F32),
            jax.ShapeDtypeStruct((NEW, 2), F32),
            jax.ShapeDtypeStruct((NEW, 2, HEAD_DIM), F32),
        ],
        in_specs=[space] * (10 + len(weights)),
        out_specs=[space] * 6,
        name="pack",
    )(*(v.reshape(1, -1) for v in scalars), tokens, *gains, *logits, *weights)


def on_device(
    tokens,
    lengths,
    memory_state,
    gain_first,
    first_gate,
    first_up,
    first_down,
    gain_mixer,
    query_weight,
    key_weight,
    value_weight,
    outgate_weight,
    beta_weight,
    decay_weight,
    decay_rate,
    decay_bias,
    head_gain,
    out_weight,
    gain_second,
    second_gate,
    second_up,
    second_down,
):
    near, far, live, rate, bias, wide_gain = pack(
        [lengths, decay_rate, decay_bias, head_gain],
        tokens,
        [gain_first, gain_mixer, gain_second],
        [beta_weight, decay_weight],
        [
            first_gate,
            first_up,
            first_down.T,
            query_weight,
            key_weight,
            value_weight,
            outgate_weight,
            out_weight.T,
            second_gate,
            second_up,
            second_down.T,
        ],
    )
    near = exchange(near, "y").reshape(128, 2048)
    far = from_others(far)
    w_up1, w_down1 = near[:, :1280], near[:, 1280:1920]
    w_mix, w_out = far[:, :1024], far[:, 1024:1280]
    w_up2, w_down2 = far[:, 1280:2560], far[:, 2560:]
    tail = near[:, 1920:]
    got = to_all(tail[:, :32].T, ("x", "c"))
    resid = got[:, 16:24].reshape(64, 128)
    gains = jnp.sum(got[0, 4:13].astype(F32).reshape(3, 3, 128), axis=0)

    def over_heads(branch):
        return jnp.sum(to_all(branch.astype(BF16), ("x", "c")).astype(F32), axis=0)

    branch = over_heads(half(resid, gains[0], w_up1, w_down1, tail))
    resid = (resid.astype(F32) + 0.5 * branch).astype(BF16)

    got = projected(resid, gains[1], w_mix, tail)
    total, small = summed(got)
    heads = total.reshape(NEW, 4, 2, HEAD_DIM)
    mixed, state_out = advance(
        heads[:, 0],
        heads[:, 1],
        heads[:, 2],
        heads[:, 3],
        small[:, 0:2],
        small[:, 2:4],
        memory_state[0],
        live,
        rate,
        bias,
        wide_gain,
    )
    mixed, state_out = lax.optimization_barrier((mixed, state_out))
    mixed = to_all(mixed, "z").reshape(64, 256)
    branch = over_heads(
        lax.dot_general(mixed, w_out, (((1,), (1,)), ((), ())), preferred_element_type=F32)
    )
    resid = (resid.astype(F32) + branch).astype(BF16)

    branch = half(resid, gains[2], w_up2, w_down2, tail)
    branch, resid = lax.optimization_barrier((branch, resid))
    both = jnp.stack([branch.astype(BF16), resid])
    both = both.reshape(2, NX * NC, 8, NY, 32).transpose(3, 1, 0, 2, 4).reshape(32, 4, 128)
    got = exchange(both, ("y", "x", "c")).reshape(NY, NX * NC, 2, 8, 32)
    branch = jnp.sum(got[:, :, 0].astype(F32), axis=1)
    out = (got[:, 0, 1].astype(F32) + 0.5 * branch).astype(BF16)
    out = out.reshape(NY, 2, NEW, 32).transpose(1, 0, 2, 3).reshape(32, 32)
    return out, state_out[None]


def solution(mesh):
    fine = Mesh(mesh.devices.reshape(NZ, NY, NX, NC), ("z", "y", "x", "c"))
    kv, tp = ("z", "y"), ("x", "c")
    in_specs = (
        P(tp, kv),
        P(kv),
        P(kv, tp, None, None),
        P(kv),
        P(kv, tp),
        P(kv, tp),
        P(tp, kv),
        P(kv),
        P(kv, tp),
        P(kv, tp),
        P(kv, tp),
        P(kv, tp),
        P(kv, None),
        P(kv, None),
        P(tp),
        P(tp),
        P(),
        P(tp, kv),
        P(kv),
        P(kv, tp),
        P(kv, tp),
        P(tp, kv),
    )
    out_specs = (P(tp, kv), P(kv, tp, None, None))
    return jax.shard_map(
        on_device, mesh=fine, in_specs=in_specs, out_specs=out_specs, check_vma=False
    )
```

```python
import jax
import jax.numpy as jnp
from jax import lax
from jax.experimental import pallas as pl
from jax.experimental.pallas import tpu as pltpu
from jax.sharding import Mesh, PartitionSpec as P

D = 2048
HEAD_DIM = 128
NEW = 4
EPS = 1e-06


NZ, NY, NX, NC = 16, 4, 4, 2
F32 = jnp.float32
BF16 = jnp.bfloat16


def exchange(x, axes):
    return lax.all_to_all(x, axes, 0, 0, tiled=True)


def to_all(x, axes):
    count = lax.axis_size(axes)
    return exchange(jnp.broadcast_to(x[None], (count, *x.shape)), axes)


def dot(a, b):
    return jnp.dot(a, b, preferred_element_type=F32)


def projected(resid, gain, weight, tail):
    wide = resid.astype(F32)
    squares = jnp.sum(wide * wide, axis=1, keepdims=True)
    operand = (wide * gain).astype(BF16)
    last = jnp.concatenate([dot(operand, tail)[:, :127], squares], axis=1)
    out = jnp.concatenate([dot(operand, weight).astype(BF16), last.astype(BF16)], axis=1)
    return exchange(out.reshape(NZ, NEW, -1), "z")


def summed(got):
    total = jnp.sum(got.astype(F32), axis=0)
    scale = lax.rsqrt(total[:, -1:] / D + EPS)
    return total[:, :-128] * scale, total[:, -128:] * scale


def half(resid, gain, w_up, w_down, tail):
    total, _ = summed(projected(resid, gain, w_up, tail))
    hidden = (jax.nn.silu(total[:, :640]) * total[:, 640:]).astype(BF16)
    hidden = to_all(hidden, "z").reshape(64, 640)
    return lax.dot_general(hidden, w_down, (((1,), (1,)), ((), ())), preferred_element_type=F32)


def advance(q, k, v, z, beta_logit, decay_logit, state_now, live, decay_rate, decay_bias, head_gain):
    query = jax.nn.silu(q)
    query = (
        query * lax.rsqrt(jnp.sum(query * query, axis=-1, keepdims=True) + EPS) * HEAD_DIM ** (-0.5)
    )
    keyvec = jax.nn.silu(k)
    keyvec = keyvec * lax.rsqrt(jnp.sum(keyvec * keyvec, axis=-1, keepdims=True) + EPS)
    values = jax.nn.silu(v)
    beta = jax.nn.sigmoid(beta_logit) * live
    decay = jnp.exp(decay_rate * jax.nn.softplus(decay_logit + decay_bias))
    outputs = []
    for t in range(NEW):
        state_now = state_now * decay[t][:, None, None]
        predicted = jnp.sum(keyvec[t][:, :, None] * state_now, axis=1)
        update = beta[t][:, None] * (values[t] - predicted)
        state_now = state_now + keyvec[t][:, :, None] * update[:, None, :]
        outputs.append(jnp.sum(query[t][:, :, None] * state_now, axis=1))
    mixed = jnp.stack(outputs, axis=0) * live[:, :, None]
    mixed = mixed * lax.rsqrt(jnp.mean(mixed * mixed, axis=-1, keepdims=True) + EPS) * head_gain
    mixed = mixed * jax.nn.silu(z)
    return mixed.reshape(NEW, -1).astype(BF16), state_now


def from_others(own):
    blocks = [own]
    for d in range(1, NY):
        blocks.append(lax.ppermute(own, "y", [(y, y ^ d) for y in range(NY)]))
    here = lax.axis_index("y")
    return jnp.concatenate([lax.select_n(here ^ y, *blocks) for y in range(NY)], axis=0)


def pack_kernel(*refs):
    length_ref, rate_ref, bias_ref, head_gain_ref, tokens_ref, *refs = refs
    gain_refs, logit_refs, weight_refs = refs[:3], refs[3:5], refs[5:-7]
    rows_ref, near_ref, far_ref, live_ref, minus_ref, wide_bias_ref, wide_gain_ref = refs[-7:]
    slot = lax.broadcasted_iota(jnp.int32, (NEW, 2), 0)
    live = (slot < jnp.broadcast_to(length_ref[...], (NEW, 2))).astype(F32)
    live_ref[...] = live
    minus_ref[...] = -rate_ref[...] * live
    wide_bias_ref[...] = jnp.broadcast_to(bias_ref[...], (NEW, 2))
    for t in range(NEW):
        wide_gain_ref[t] = jnp.broadcast_to(head_gain_ref[...], (2, HEAD_DIM))
    at = 0
    for ref in weight_refs[2:]:
        far_ref[:, at : at + ref.shape[1]] = ref[...]
        at += ref.shape[1]
    near_ref[:, :640] = weight_refs[0][...]
    near_ref[:, 640:1280] = weight_refs[1][...]
    device = NC * lax.axis_index("x") + lax.axis_index("c")
    row = lax.broadcasted_iota(jnp.int32, (16, 32), 0)
    logits = []
    for ref in logit_refs:
        block = ref[...].astype(F32)
        for h in range(2):
            mine = jnp.where(row == 2 * device + h, block, 0.0)
            logits.append(jnp.sum(mine, axis=0, keepdims=True))
    tail = jnp.concatenate([*logits, jnp.zeros((124, 32), F32)], axis=0)
    near_ref[:, 1280:] = tail.T.astype(BF16)
    gains = jnp.concatenate([ref[...] for ref in gain_refs], axis=0)
    first = gains.astype(BF16).astype(F32)
    second = (gains - first).astype(BF16).astype(F32)
    third = gains - first - second
    gap = jnp.zeros((7, 32), F32)
    small = jnp.concatenate([first, second, third, gap], axis=0)
    rows = tokens_ref[...].astype(F32)
    lane = lax.broadcasted_iota(jnp.int32, (24, 128), 1)
    here = lane // 32 == lax.axis_index("y")
    for y in range(NY):
        mine = [rows[4 * y : 4 * y + 4], rows[16 + 4 * y : 20 + 4 * y]]
        block = jnp.concatenate([*mine, small], axis=0)
        block = jnp.concatenate([block] * NY, axis=1)
        block = jnp.where(here, block, 0.0).astype(BF16)
        for i in range(NX * NC):
            rows_ref[y * NX * NC + i] = block


def pack(scalars, tokens, gains, logits, weights):
    gains = [g.reshape(1, 32) for g in gains]
    logits = [w.T for w in logits]
    space = pl.BlockSpec(memory_space=pltpu.VMEM)
    return pl.pallas_call(
        pack_kernel,
        out_shape=[
            jax.ShapeDtypeStruct((NY * NX * NC, 24, 128), BF16),
            jax.ShapeDtypeStruct((32, 1408), BF16),
            jax.ShapeDtypeStruct((32, 3840), BF16),
            jax.ShapeDtypeStruct((NEW, 2), F32),
            jax.ShapeDtypeStruct((NEW, 2), F32),
            jax.ShapeDtypeStruct((NEW, 2), F32),
            jax.ShapeDtypeStruct((NEW, 2, HEAD_DIM), F32),
        ],
        in_specs=[space] * (10 + len(weights)),
        out_specs=[space] * 7,
        name="pack",
    )(*(v.reshape(1, -1) for v in scalars), tokens, *gains, *logits, *weights)


def on_device(
    tokens,
    lengths,
    memory_state,
    gain_first,
    first_gate,
    first_up,
    first_down,
    gain_mixer,
    query_weight,
    key_weight,
    value_weight,
    outgate_weight,
    beta_weight,
    decay_weight,
    decay_rate,
    decay_bias,
    head_gain,
    out_weight,
    gain_second,
    second_gate,
    second_up,
    second_down,
):
    rows, near, far, live, rate, bias, wide_gain = pack(
        [lengths, decay_rate, decay_bias, head_gain],
        tokens,
        [gain_first, gain_mixer, gain_second],
        [beta_weight, decay_weight],
        [
            first_gate,
            first_up,
            first_down.T,
            query_weight,
            key_weight,
            value_weight,
            outgate_weight,
            out_weight.T,
            second_gate,
            second_up,
            second_down.T,
        ],
    )
    rows = exchange(rows, ("y", "x", "c")).reshape(NY, NX * NC, 24, 128)
    rows = jnp.sum(rows.astype(F32), axis=0)
    resid = rows[:, :8].reshape(64, 128).astype(BF16)
    gains = jnp.sum(rows[0, 8:17].reshape(3, 3, 128), axis=0)
    near = from_others(near)
    far = from_others(far)
    w_up1, w_down1 = near[:, :1280], far[:, :640]
    w_mix, w_out = far[:, 640:1664], far[:, 1664:1920]
    w_up2, w_down2 = far[:, 1920:3200], far[:, 3200:]
    tail = near[:, 1280:]

    def over_heads(branch):
        return jnp.sum(to_all(branch.astype(BF16), ("x", "c")).astype(F32), axis=0)

    branch = half(resid, gains[0], w_up1, w_down1, tail)
    branch = over_heads(branch)
    resid = (resid.astype(F32) + 0.5 * branch).astype(BF16)

    got = projected(resid, gains[1], w_mix, tail)
    total, small = summed(got)
    heads = total.reshape(NEW, 4, 2, HEAD_DIM)
    mixed, state_out = advance(
        heads[:, 0],
        heads[:, 1],
        heads[:, 2],
        heads[:, 3],
        small[:, 0:2],
        small[:, 2:4],
        memory_state[0],
        live,
        rate,
        bias,
        wide_gain,
    )
    mixed, state_out = lax.optimization_barrier((mixed, state_out))
    mixed = to_all(mixed, "z").reshape(64, 256)
    branch = over_heads(
        lax.dot_general(mixed, w_out, (((1,), (1,)), ((), ())), preferred_element_type=F32)
    )
    resid = (resid.astype(F32) + branch).astype(BF16)

    branch = half(resid, gains[2], w_up2, w_down2, tail)
    branch, resid = lax.optimization_barrier((branch, resid))
    both = jnp.stack([branch.astype(BF16), resid])
    both = both.reshape(2, NX * NC, 8, NY, 32).transpose(3, 1, 0, 2, 4).reshape(32, 4, 128)
    got = exchange(both, ("y", "x", "c")).reshape(NY, NX * NC, 2, 8, 32)
    branch = jnp.sum(got[:, :, 0].astype(F32), axis=1)
    out = (got[:, 0, 1].astype(F32) + 0.5 * branch).astype(BF16)
    out = out.reshape(NY, 2, NEW, 32).transpose(1, 0, 2, 3).reshape(32, 32)
    return out, state_out[None]


def solution(mesh):
    fine = Mesh(mesh.devices.reshape(NZ, NY, NX, NC), ("z", "y", "x", "c"))
    kv, tp = ("z", "y"), ("x", "c")
    in_specs = (
        P(tp, kv),
        P(kv),
        P(kv, tp, None, None),
        P(kv),
        P(kv, tp),
        P(kv, tp),
        P(tp, kv),
        P(kv),
        P(kv, tp),
        P(kv, tp),
        P(kv, tp),
        P(kv, tp),
        P(kv, None),
        P(kv, None),
        P(tp),
        P(tp),
        P(),
        P(tp, kv),
        P(kv),
        P(kv, tp),
        P(kv, tp),
        P(tp, kv),
    )
    out_specs = (P(tp, kv), P(kv, tp, None, None))
    return jax.shard_map(
        on_device, mesh=fine, in_specs=in_specs, out_specs=out_specs, check_vma=False
    )
```

```python
import jax
import jax.numpy as jnp
from jax import lax
from jax.experimental import pallas as pl
from jax.experimental.pallas import tpu as pltpu
from jax.sharding import Mesh, PartitionSpec as P

D = 2048
HEAD_DIM = 128
NEW = 4
EPS = 1e-06


NZ, NY, NX, NC = 16, 4, 4, 2
F32 = jnp.float32
BF16 = jnp.bfloat16


def exchange(x, axes):
    return lax.all_to_all(x, axes, 0, 0, tiled=True)


def to_all(x, axes):
    count = lax.axis_size(axes)
    return exchange(jnp.broadcast_to(x[None], (count, *x.shape)), axes)


def dot(a, b):
    return jnp.dot(a, b, preferred_element_type=F32)


def projected(resid, gain, weight, tail):
    wide = resid.astype(F32)
    squares = jnp.sum(wide * wide, axis=1, keepdims=True)
    operand = (wide * gain).astype(BF16)
    last = jnp.concatenate([dot(operand, tail)[:, :127], squares], axis=1)
    out = jnp.concatenate([dot(operand, weight).astype(BF16), last.astype(BF16)], axis=1)
    return exchange(out.reshape(NZ, NEW, -1), "z")


def summed(got):
    total = jnp.sum(got.astype(F32), axis=0)
    scale = lax.rsqrt(total[:, -1:] / D + EPS)
    return total[:, :-128] * scale, total[:, -128:] * scale


def half(resid, gain, w_up, w_down, tail):
    total, _ = summed(projected(resid, gain, w_up, tail))
    hidden = (jax.nn.silu(total[:, :640]) * total[:, 640:]).astype(BF16)
    hidden = to_all(hidden, "z").reshape(64, 640)
    return lax.dot_general(hidden, w_down, (((1,), (1,)), ((), ())), preferred_element_type=F32)


def advance(q, k, v, z, beta_logit, decay_logit, state_now, live, decay_rate, decay_bias, head_gain):
    query = jax.nn.silu(q)
    query = (
        query * lax.rsqrt(jnp.sum(query * query, axis=-1, keepdims=True) + EPS) * HEAD_DIM ** (-0.5)
    )
    keyvec = jax.nn.silu(k)
    keyvec = keyvec * lax.rsqrt(jnp.sum(keyvec * keyvec, axis=-1, keepdims=True) + EPS)
    values = jax.nn.silu(v)
    beta = jax.nn.sigmoid(beta_logit) * live
    decay = jnp.exp(decay_rate * jax.nn.softplus(decay_logit + decay_bias))
    outputs = []
    for t in range(NEW):
        state_now = state_now * decay[t][:, None, None]
        predicted = jnp.sum(keyvec[t][:, :, None] * state_now, axis=1)
        update = beta[t][:, None] * (values[t] - predicted)
        state_now = state_now + keyvec[t][:, :, None] * update[:, None, :]
        outputs.append(jnp.sum(query[t][:, :, None] * state_now, axis=1))
    mixed = jnp.stack(outputs, axis=0) * live[:, :, None]
    mixed = mixed * lax.rsqrt(jnp.mean(mixed * mixed, axis=-1, keepdims=True) + EPS) * head_gain
    mixed = mixed * jax.nn.silu(z)
    return mixed.reshape(NEW, -1).astype(BF16), state_now


def from_others(own):
    blocks = [own]
    for d in range(1, NY):
        blocks.append(lax.ppermute(own, "y", [(y, y ^ d) for y in range(NY)]))
    here = lax.axis_index("y")
    return jnp.concatenate([lax.select_n(here ^ y, *blocks) for y in range(NY)], axis=0)


def pack_kernel(*refs):
    tokens_ref, *refs = refs
    gain_refs, logit_refs, weight_refs, out_ref = refs[:3], refs[3:5], refs[5:-1], refs[-1]
    at = 0
    for ref in weight_refs:
        block = ref[...]
        for y in range(NY):
            out_ref[y, :, at : at + block.shape[1]] = block
        at += block.shape[1]
    gains = jnp.concatenate([ref[...] for ref in gain_refs], axis=0)
    first = gains.astype(BF16).astype(F32)
    second = (gains - first).astype(BF16).astype(F32)
    third = gains - first - second
    device = NC * lax.axis_index("x") + lax.axis_index("c")
    row = lax.broadcasted_iota(jnp.int32, (16, 32), 0)
    logits = []
    for ref in logit_refs:
        block = ref[...].astype(F32)
        for h in range(2):
            mine = jnp.where(row == 2 * device + h, block, 0.0)
            logits.append(jnp.sum(mine, axis=0, keepdims=True))
    gap = jnp.zeros((3, 32), F32)
    small = jnp.concatenate([*logits, first, second, third, gap], axis=0)
    rows = tokens_ref[...].astype(F32)
    end = jnp.zeros((104, 32), F32)
    for y in range(NY):
        mine = [rows[4 * y : 4 * y + 4], rows[16 + 4 * y : 20 + 4 * y]]
        tail = jnp.concatenate([small, *mine, end], axis=0)
        out_ref[y, :, at:] = tail.T.astype(BF16)


def pack_far_kernel(length_ref, rate_ref, bias_ref, head_gain_ref, *refs):
    weight_refs = refs[:-5]
    far_ref, live_ref, minus_ref, wide_bias_ref, wide_gain_ref = refs[-5:]
    slot = lax.broadcasted_iota(jnp.int32, (NEW, 2), 0)
    live = (slot < jnp.broadcast_to(length_ref[...], (NEW, 2))).astype(F32)
    live_ref[...] = live
    minus_ref[...] = -rate_ref[...] * live
    wide_bias_ref[...] = jnp.broadcast_to(bias_ref[...], (NEW, 2))
    for t in range(NEW):
        wide_gain_ref[t] = jnp.broadcast_to(head_gain_ref[...], (2, HEAD_DIM))
    at = 0
    for ref in weight_refs:
        far_ref[:, at : at + ref.shape[1]] = ref[...]
        at += ref.shape[1]


def pack(tokens, gains, logits, weights):
    gains = [g.reshape(1, 32) for g in gains]
    logits = [w.T for w in logits]
    space = pl.BlockSpec(memory_space=pltpu.VMEM)
    return pl.pallas_call(
        pack_kernel,
        out_shape=jax.ShapeDtypeStruct((NY, 32, 1408), BF16),
        in_specs=[space] * (6 + len(weights)),
        out_specs=space,
        name="pack",
    )(tokens, *gains, *logits, *weights)


def pack_far(scalars, weights):
    space = pl.BlockSpec(memory_space=pltpu.VMEM)
    return pl.pallas_call(
        pack_far_kernel,
        out_shape=[
            jax.ShapeDtypeStruct((32, 3840), BF16),
            jax.ShapeDtypeStruct((NEW, 2), F32),
            jax.ShapeDtypeStruct((NEW, 2), F32),
            jax.ShapeDtypeStruct((NEW, 2), F32),
            jax.ShapeDtypeStruct((NEW, 2, HEAD_DIM), F32),
        ],
        in_specs=[space] * (4 + len(weights)),
        out_specs=[space] * 5,
        name="pack_far",
    )(*(v.reshape(1, -1) for v in scalars), *weights)


def on_device(
    tokens,
    lengths,
    memory_state,
    gain_first,
    first_gate,
    first_up,
    first_down,
    gain_mixer,
    query_weight,
    key_weight,
    value_weight,
    outgate_weight,
    beta_weight,
    decay_weight,
    decay_rate,
    decay_bias,
    head_gain,
    out_weight,
    gain_second,
    second_gate,
    second_up,
    second_down,
):
    near = pack(
        tokens,
        [gain_first, gain_mixer, gain_second],
        [beta_weight, decay_weight],
        [first_gate, first_up],
    )
    far, live, rate, bias, wide_gain = pack_far(
        [lengths, decay_rate, decay_bias, head_gain],
        [
            first_down.T,
            query_weight,
            key_weight,
            value_weight,
            outgate_weight,
            out_weight.T,
            second_gate,
            second_up,
            second_down.T,
        ],
    )
    near = exchange(near, "y").reshape(128, 1408)
    far = from_others(far)
    w_up1, w_down1 = near[:, :1280], far[:, :640]
    w_mix, w_out = far[:, 640:1664], far[:, 1664:1920]
    w_up2, w_down2 = far[:, 1920:3200], far[:, 3200:]
    tail = near[:, 1280:]
    got = to_all(tail[:, :32].T, ("x", "c"))
    resid = got[:, 16:24].reshape(64, 128)
    gains = jnp.sum(got[0, 4:13].astype(F32).reshape(3, 3, 128), axis=0)

    def over_heads(branch):
        return jnp.sum(to_all(branch.astype(BF16), ("x", "c")).astype(F32), axis=0)

    branch = half(resid, gains[0], w_up1, w_down1, tail)
    branch = over_heads(branch)
    resid = (resid.astype(F32) + 0.5 * branch).astype(BF16)

    got = projected(resid, gains[1], w_mix, tail)
    total, small = summed(got)
    heads = total.reshape(NEW, 4, 2, HEAD_DIM)
    mixed, state_out = advance(
        heads[:, 0],
        heads[:, 1],
        heads[:, 2],
        heads[:, 3],
        small[:, 0:2],
        small[:, 2:4],
        memory_state[0],
        live,
        rate,
        bias,
        wide_gain,
    )
    mixed, state_out = lax.optimization_barrier((mixed, state_out))
    mixed = to_all(mixed, "z").reshape(64, 256)
    branch = over_heads(
        lax.dot_general(mixed, w_out, (((1,), (1,)), ((), ())), preferred_element_type=F32)
    )
    resid = (resid.astype(F32) + branch).astype(BF16)

    branch = half(resid, gains[2], w_up2, w_down2, tail)
    branch, resid = lax.optimization_barrier((branch, resid))
    both = jnp.stack([branch.astype(BF16), resid])
    both = both.reshape(2, NX * NC, 8, NY, 32).transpose(3, 1, 0, 2, 4).reshape(32, 4, 128)
    got = exchange(both, ("y", "x", "c")).reshape(NY, NX * NC, 2, 8, 32)
    branch = jnp.sum(got[:, :, 0].astype(F32), axis=1)
    out = (got[:, 0, 1].astype(F32) + 0.5 * branch).astype(BF16)
    out = out.reshape(NY, 2, NEW, 32).transpose(1, 0, 2, 3).reshape(32, 32)
    return out, state_out[None]


def solution(mesh):
    fine = Mesh(mesh.devices.reshape(NZ, NY, NX, NC), ("z", "y", "x", "c"))
    kv, tp = ("z", "y"), ("x", "c")
    in_specs = (
        P(tp, kv),
        P(kv),
        P(kv, tp, None, None),
        P(kv),
        P(kv, tp),
        P(kv, tp),
        P(tp, kv),
        P(kv),
        P(kv, tp),
        P(kv, tp),
        P(kv, tp),
        P(kv, tp),
        P(kv, None),
        P(kv, None),
        P(tp),
        P(tp),
        P(),
        P(tp, kv),
        P(kv),
        P(kv, tp),
        P(kv, tp),
        P(tp, kv),
    )
    out_specs = (P(tp, kv), P(kv, tp, None, None))
    return jax.shard_map(
        on_device, mesh=fine, in_specs=in_specs, out_specs=out_specs, check_vma=False
    )
```

```python
import jax
import jax.numpy as jnp
from jax import lax
from jax.experimental import pallas as pl
from jax.experimental.pallas import tpu as pltpu
from jax.sharding import Mesh, PartitionSpec as P

D = 2048
HEAD_DIM = 128
NEW = 4
EPS = 1e-06


NZ, NY, NX, NC = 16, 4, 4, 2
F32 = jnp.float32
BF16 = jnp.bfloat16


def exchange(x, axes):
    return lax.all_to_all(x, axes, 0, 0, tiled=True)


def to_all(x, axes):
    count = lax.axis_size(axes)
    return exchange(jnp.broadcast_to(x[None], (count, *x.shape)), axes)


def dot(a, b):
    return jnp.dot(a, b, preferred_element_type=F32)


def projected(resid, gain, weight, tail):
    wide = resid.astype(F32)
    squares = jnp.sum(wide * wide, axis=1, keepdims=True)
    operand = (wide * gain).astype(BF16)
    last = jnp.concatenate([dot(operand, tail)[:, :127], squares], axis=1)
    out = jnp.concatenate([dot(operand, weight).astype(BF16), last.astype(BF16)], axis=1)
    return exchange(out.reshape(NZ, NEW, -1), "z")


def summed(got):
    total = jnp.sum(got.astype(F32), axis=0)
    scale = lax.rsqrt(total[:, -1:] / D + EPS)
    return total[:, :-128] * scale, total[:, -128:] * scale


def half(resid, gain, w_up, w_down, tail):
    total, _ = summed(projected(resid, gain, w_up, tail))
    hidden = (jax.nn.silu(total[:, :640]) * total[:, 640:]).astype(BF16)
    hidden = to_all(hidden, "z").reshape(64, 640)
    return lax.dot_general(hidden, w_down, (((1,), (1,)), ((), ())), preferred_element_type=F32)


def advance(q, k, v, z, beta_logit, decay_logit, state_now, live, decay_rate, decay_bias, head_gain):
    query = jax.nn.silu(q)
    query = (
        query * lax.rsqrt(jnp.sum(query * query, axis=-1, keepdims=True) + EPS) * HEAD_DIM ** (-0.5)
    )
    keyvec = jax.nn.silu(k)
    keyvec = keyvec * lax.rsqrt(jnp.sum(keyvec * keyvec, axis=-1, keepdims=True) + EPS)
    values = jax.nn.silu(v)
    beta = jax.nn.sigmoid(beta_logit) * live
    decay = jnp.exp(decay_rate * jax.nn.softplus(decay_logit + decay_bias))
    outputs = []
    for t in range(NEW):
        state_now = state_now * decay[t][:, None, None]
        predicted = jnp.sum(keyvec[t][:, :, None] * state_now, axis=1)
        update = beta[t][:, None] * (values[t] - predicted)
        state_now = state_now + keyvec[t][:, :, None] * update[:, None, :]
        outputs.append(jnp.sum(query[t][:, :, None] * state_now, axis=1))
    mixed = jnp.stack(outputs, axis=0) * live[:, :, None]
    mixed = mixed * lax.rsqrt(jnp.mean(mixed * mixed, axis=-1, keepdims=True) + EPS) * head_gain
    mixed = mixed * jax.nn.silu(z)
    return mixed.reshape(NEW, -1).astype(BF16), state_now


def from_others(own):
    blocks = [own]
    for d in range(1, NY):
        blocks.append(lax.ppermute(own, "y", [(y, y ^ d) for y in range(NY)]))
    here = lax.axis_index("y")
    return jnp.concatenate([lax.select_n(here ^ y, *blocks) for y in range(NY)], axis=0)


def pack_kernel(*refs):
    length_ref, rate_ref, bias_ref, head_gain_ref, tokens_ref, *refs = refs
    gain_refs, logit_refs, weight_refs = refs[:3], refs[3:5], refs[5:-6]
    out_ref, far_ref, live_ref, minus_ref, wide_bias_ref, wide_gain_ref = refs[-6:]
    slot = lax.broadcasted_iota(jnp.int32, (NEW, 2), 0)
    live = (slot < jnp.broadcast_to(length_ref[...], (NEW, 2))).astype(F32)
    live_ref[...] = live
    minus_ref[...] = -rate_ref[...] * live
    wide_bias_ref[...] = jnp.broadcast_to(bias_ref[...], (NEW, 2))
    for t in range(NEW):
        wide_gain_ref[t] = jnp.broadcast_to(head_gain_ref[...], (2, HEAD_DIM))
    at = 0
    for ref in weight_refs[2:]:
        far_ref[:, at : at + ref.shape[1]] = ref[...]
        at += ref.shape[1]
    at = 0
    for ref in weight_refs[:2]:
        block = ref[...]
        for y in range(NY):
            out_ref[y, :, at : at + block.shape[1]] = block
        at += block.shape[1]
    gains = jnp.concatenate([ref[...] for ref in gain_refs], axis=0)
    first = gains.astype(BF16).astype(F32)
    second = (gains - first).astype(BF16).astype(F32)
    third = gains - first - second
    device = NC * lax.axis_index("x") + lax.axis_index("c")
    row = lax.broadcasted_iota(jnp.int32, (16, 32), 0)
    logits = []
    for ref in logit_refs:
        block = ref[...].astype(F32)
        for h in range(2):
            mine = jnp.where(row == 2 * device + h, block, 0.0)
            logits.append(jnp.sum(mine, axis=0, keepdims=True))
    gap = jnp.zeros((3, 32), F32)
    small = jnp.concatenate([*logits, first, second, third, gap], axis=0)
    rows = tokens_ref[...].astype(F32)
    end = jnp.zeros((104, 32), F32)
    for y in range(NY):
        mine = [rows[4 * y : 4 * y + 4], rows[16 + 4 * y : 20 + 4 * y]]
        tail = jnp.concatenate([small, *mine, end], axis=0)
        out_ref[y, :, at:] = tail.T.astype(BF16)


def pack(scalars, tokens, gains, logits, weights):
    gains = [g.reshape(1, 32) for g in gains]
    logits = [w.T for w in logits]
    space = pl.BlockSpec(memory_space=pltpu.VMEM)
    return pl.pallas_call(
        pack_kernel,
        out_shape=[
            jax.ShapeDtypeStruct((NY, 32, 1408), BF16),
            jax.ShapeDtypeStruct((32, 3840), BF16),
            jax.ShapeDtypeStruct((NEW, 2), F32),
            jax.ShapeDtypeStruct((NEW, 2), F32),
            jax.ShapeDtypeStruct((NEW, 2), F32),
            jax.ShapeDtypeStruct((NEW, 2, HEAD_DIM), F32),
        ],
        in_specs=[space] * (10 + len(weights)),
        out_specs=[space] * 6,
        name="pack",
    )(*(v.reshape(1, -1) for v in scalars), tokens, *gains, *logits, *weights)


def on_device(
    tokens,
    lengths,
    memory_state,
    gain_first,
    first_gate,
    first_up,
    first_down,
    gain_mixer,
    query_weight,
    key_weight,
    value_weight,
    outgate_weight,
    beta_weight,
    decay_weight,
    decay_rate,
    decay_bias,
    head_gain,
    out_weight,
    gain_second,
    second_gate,
    second_up,
    second_down,
):
    near, far, live, rate, bias, wide_gain = pack(
        [lengths, decay_rate, decay_bias, head_gain],
        tokens,
        [gain_first, gain_mixer, gain_second],
        [beta_weight, decay_weight],
        [
            first_gate,
            first_up,
            first_down.T,
            query_weight,
            key_weight,
            value_weight,
            outgate_weight,
            out_weight.T,
            second_gate,
            second_up,
            second_down.T,
        ],
    )
    near = exchange(near, "y").reshape(128, 1408)
    far = from_others(far)
    w_up1, w_down1 = near[:, :1280], far[:, :640]
    w_mix, w_out = far[:, 640:1664], far[:, 1664:1920]
    w_up2, w_down2 = far[:, 1920:3200], far[:, 3200:]
    tail = near[:, 1280:]
    got = to_all(tail[:, :32].T, ("x", "c"))
    resid = got[:, 16:24].reshape(64, 128)
    gains = jnp.sum(got[0, 4:13].astype(F32).reshape(3, 3, 128), axis=0)

    def over_heads(branch):
        return jnp.sum(to_all(branch.astype(BF16), ("x", "c")).astype(F32), axis=0)

    branch = half(resid, gains[0], w_up1, w_down1, tail)
    branch = over_heads(branch)
    resid = (resid.astype(F32) + 0.5 * branch).astype(BF16)

    got = projected(resid, gains[1], w_mix, tail)
    total, small = summed(got)
    heads = total.reshape(NEW, 4, 2, HEAD_DIM)
    mixed, state_out = advance(
        heads[:, 0],
        heads[:, 1],
        heads[:, 2],
        heads[:, 3],
        small[:, 0:2],
        small[:, 2:4],
        memory_state[0],
        live,
        rate,
        bias,
        wide_gain,
    )
    mixed, state_out = lax.optimization_barrier((mixed, state_out))
    mixed = to_all(mixed, "z").reshape(64, 256)
    branch = over_heads(
        lax.dot_general(mixed, w_out, (((1,), (1,)), ((), ())), preferred_element_type=F32)
    )
    resid = (resid.astype(F32) + branch).astype(BF16)

    branch = half(resid, gains[2], w_up2, w_down2, tail)
    branch, resid = lax.optimization_barrier((branch, resid))
    both = jnp.stack([branch.astype(BF16), resid])
    both = both.reshape(2, NX * NC, 8, NY, 32).transpose(3, 1, 0, 2, 4).reshape(32, 4, 128)
    got = exchange(both, ("y", "x", "c")).reshape(NY, NX * NC, 2, 8, 32)
    branch = jnp.sum(got[:, :, 0].astype(F32), axis=1)
    out = (got[:, 0, 1].astype(F32) + 0.5 * branch).astype(BF16)
    out = out.reshape(NY, 2, NEW, 32).transpose(1, 0, 2, 3).reshape(32, 32)
    return out, state_out[None]


def solution(mesh):
    fine = Mesh(mesh.devices.reshape(NZ, NY, NX, NC), ("z", "y", "x", "c"))
    kv, tp = ("z", "y"), ("x", "c")
    in_specs = (
        P(tp, kv),
        P(kv),
        P(kv, tp, None, None),
        P(kv),
        P(kv, tp),
        P(kv, tp),
        P(tp, kv),
        P(kv),
        P(kv, tp),
        P(kv, tp),
        P(kv, tp),
        P(kv, tp),
        P(kv, None),
        P(kv, None),
        P(tp),
        P(tp),
        P(),
        P(tp, kv),
        P(kv),
        P(kv, tp),
        P(kv, tp),
        P(tp, kv),
    )
    out_specs = (P(tp, kv), P(kv, tp, None, None))
    return jax.shard_map(
        on_device, mesh=fine, in_specs=in_specs, out_specs=out_specs, check_vma=False
    )
```
